256 devices in a mesh: ep: 64 (over z, x, core), tp: 4 (over y).
Axes of the slice: x: 4, y: 4, z: 8, core: 2. Of those that a mesh axis runs over, the one named last changes fastest.
Arguments:
- projected_queries: bfloat16 [16384, 2048], P('ep', 'tp'), may hold values from -245 to 245, as said below
- key_proj: bfloat16 [16384, 512], P('ep', 'tp'), may hold values from -6.2 to 6.2
- projected_values: bfloat16 [16384, 512], P('ep', 'tp'), may hold values from -24 to 24
- head_sink_logits: float32 [32], P('tp'), may hold values from 1 to 6
- out_weight: bfloat16 [2048, 4096], P('tp'), may hold values from -0.125 to 0.125
- expert_input: bfloat16 [8192, 4096], P('ep'), may hold values from -6 to 6
- norm_gain: float32 [4096], replicated, may hold values from 0.1 to 1.9
- routing: int32 [8192, 4], P('ep'), may hold values from 0 to 63, all different within a row; in each aligned block of 128 rows (0 to 127, 128 to 255, ...) at most 12 rows name the same one
- route_weight: float32 [8192, 4], P('ep'), may hold values from 0.1 to 1
- gate_weight: bfloat16 [64, 4096, 1024], P('ep', None, 'tp'), may hold values from -0.27929688 to 0.27929688
- up_weight: bfloat16 [64, 4096, 1024], P('ep', None, 'tp'), may hold values from -0.27929688 to 0.27929688
- down_weight: bfloat16 [64, 1024, 4096], P('ep', 'tp'), may hold values from -0.046875 to 0.046875
Outputs:
- mixer_output: bfloat16 [16384, 4096], P(('ep', 'tp'))
- expert_output: bfloat16 [8192, 4096], P('ep', 'tp')
The draws below stay inside these ranges and needn't reach their ends.
Inputs may be any that keep to these rules, and one draw needn't show every extreme that they name: `projected_queries`: in the hidden draw some queries nearly equal a large multiple of a nearby key. `routing`: each row names 4 different experts; among the rows of one device (aligned blocks of 128 rows) no expert is named more than 12 times, a bound that some block reaches.
All inputs are finite; a program needn't handle non-finite values.
Results may differ from the reference program's by a relative error of at most 0.014.
Values may be sent and summed in bfloat16 or wider, within the bound.
A program may use at most 128 MiB of HBM per device.

```python
import math
import jax
import jax.numpy as jnp
import numpy as np
from jax import lax

D = 4096
QUERY_HEADS = 32
KEY_VALUE_HEADS = 8
HEAD_SIZE = 64
WINDOW_KEYS = 128
FF = 1024
TOPK = 4
TOK_B_DEV = 128
EXPERTS = 64
CAP = 12
ATTENTION_TOKENS = 16384
TOKENS_B = 8192
N_EP = 64
N_TP = 4


def plant_pair(key):
    base = jax.random.fold_in(key, 17)
    leading_key, following_key = jax.random.split(base, 2)
    sampled_keys = jnp.clip(jax.random.normal(following_key, (ATTENTION_TOKENS, KEY_VALUE_HEADS, HEAD_SIZE), jnp.float32), -6.0, 6.0)
    query_vectors = jnp.clip(jax.random.normal(leading_key, (ATTENTION_TOKENS, KEY_VALUE_HEADS, QUERY_HEADS // KEY_VALUE_HEADS, HEAD_SIZE), jnp.float32), -6.0, 6.0)
    return (query_vectors.reshape(ATTENTION_TOKENS, QUERY_HEADS * HEAD_SIZE), sampled_keys.reshape(ATTENTION_TOKENS, KEY_VALUE_HEADS * HEAD_SIZE))


def draw_projected_queries(key, part):
    return plant_pair(key)[0].astype(jnp.bfloat16)


def draw_key_proj(key, part):
    return plant_pair(key)[1].astype(jnp.bfloat16)


def block_scale(own_key, extent, cuts, smallest, largest):
    factor_of, own = 1.0, jax.random.fold_in(own_key, 6)
    for dim, shards_of in cuts:
        draws = jnp.exp(jax.random.uniform(jax.random.fold_in(own, dim), (shards_of,), jnp.float32, smallest / len(cuts), largest / len(cuts)))
        factor_of = factor_of * jnp.repeat(draws, extent[dim] // shards_of).reshape([-1 if axis == dim else 1 for axis in range(len(extent))])
    return factor_of


def assign_block(key, own, number, rows, number_of, top, bound, skew):
    sequence = jax.random.permutation(key, number_of)
    heavy_load, common = shares(number_of, rows * top, bound, skew, True), shares(number_of, rows * top, bound, skew, False)
    places = jnp.arange(number_of)

    def named(tallies, rotation):
        used = int((tallies > 0).sum())
        fixed = max(1, used // 4)
        moved = fixed + (places - fixed + rotation * (used - fixed)) % max(1, number_of - fixed)
        return jnp.zeros((number_of,), jnp.int32).at[sequence[jnp.where(places < fixed, places, moved)]].set(jnp.asarray(tallies, jnp.int32))

    tallies = jnp.where(number % 4 == 0, named(heavy_load, number // 4), named(common, number - number // 4 - 1))
    mixed = jax.random.permutation(jax.random.fold_in(own, 3), number_of)
    giver, taker = mixed[0:number_of // 2 * 2:2], mixed[1:number_of // 2 * 2:2]
    room = jnp.minimum(tallies[giver] - 1, bound - tallies[taker]) // 2
    room = jnp.where((giver == sequence[0]) | (taker == sequence[0]) | (tallies[taker] == 0), 0, jnp.maximum(room, 0))
    moved = jax.random.randint(jax.random.fold_in(own, 4), (number_of // 2,), 0, 1 << 20) % (room + 1)
    tallies = tallies.at[giver].add(-moved).at[taker].add(moved)
    items = jnp.searchsorted(jnp.cumsum(tallies), jnp.arange(rows * top), side="right").astype(jnp.int32)
    table = items.reshape(top, rows).T
    table = table[jax.random.permutation(jax.random.fold_in(own, 1), rows)]
    rotation = jax.random.randint(jax.random.fold_in(own, 2), (rows, 1), 0, top)
    return jnp.take_along_axis(table, (jnp.arange(top)[None, :] + rotation) % top, axis=1)


def shares(number_of, total, limit, slope, full):
    loads = [(1 << 20) // math.isqrt(rank ** slope) + 1 for rank in range(1, number_of + 1)]
    largest = limit if full else min(limit, max(-(-total // number_of), total * loads[0] // sum(loads)))
    least = 1 if total - largest >= number_of - 1 else 0
    holding, surplus = [largest] + [least] * (number_of - 1), total - largest - least * (number_of - 1)
    while surplus > 0:
        free = [i for i in range(1, number_of) if holding[i] < largest] or [i for i in range(1, number_of) if holding[i] < limit]
        pool, remaining = sum([loads[i] for i in free]), surplus
        for i in free:
            more = min(limit - holding[i], max(1, remaining * loads[i] // pool), surplus)
            holding[i] = holding[i] + more
            surplus = surplus - more
    return np.array(holding)


def scatter_about(stream_key, shape, scale, bound, cuts=(), held_as=jnp.bfloat16):
    gain = block_scale(stream_key, shape, cuts, -0.22, 0.18) if cuts else 1.0
    drawn = jax.random.normal(stream_key, shape, jnp.float32) * scale * gain
    return jnp.minimum(jnp.maximum(drawn, -bound), bound).astype(held_as)


def setup_inputs(seed: int = 0) -> dict:
    arg_keys = jax.random.split(jax.random.key(seed), 13)
    projected_queries = draw_projected_queries(jax.random.fold_in(arg_keys[12], 71), 0)
    key_proj = draw_key_proj(jax.random.fold_in(arg_keys[12], 71), 0)
    projected_values = scatter_about(arg_keys[2], (ATTENTION_TOKENS, KEY_VALUE_HEADS * HEAD_SIZE), 4.0, 24.0, ((0, 64), (1, 4)))
    head_sink_logits = jnp.clip(1.0 + 5.0 * jax.random.uniform(arg_keys[3], (QUERY_HEADS,), jnp.float32) ** block_scale(arg_keys[3], (QUERY_HEADS,), ((0, 4),), -0.2, 0.2), 1.0, 6.0)
    out_weight = scatter_about(arg_keys[4], (QUERY_HEADS * HEAD_SIZE, D), (QUERY_HEADS * HEAD_SIZE) ** -0.5, 0.125, ((0, 4),))
    expert_input = scatter_about(arg_keys[5], (TOKENS_B, D), 1.0, 6.0, ((0, 64),))
    norm_gain = jnp.clip(1.0 + 0.18 * jax.random.normal(arg_keys[6], (D,), jnp.float32), 0.1, 1.9)
    routing_keys = jax.random.split(jax.random.fold_in(arg_keys[7], 1), TOKENS_B // TOK_B_DEV)
    routing_turns = jax.random.permutation(jax.random.fold_in(arg_keys[7], 3), TOKENS_B // TOK_B_DEV)
    routing = jax.vmap(lambda own, number: assign_block(jax.random.fold_in(arg_keys[7], 2), own, number, TOK_B_DEV, N_EP, TOPK, CAP, 2))(routing_keys, routing_turns).reshape((TOKENS_B, TOPK))
    route_weight = jnp.clip(jnp.exp(math.log(1.0) - 2.3025851 * jax.random.uniform(arg_keys[8], (TOKENS_B, TOPK), jnp.float32) ** block_scale(arg_keys[8], (TOKENS_B, TOPK), ((0, 64),), -0.2, 0.2)), 0.1, 1.0)
    gate_weight = scatter_about(arg_keys[9], (EXPERTS, D, FF), 0.046875, 0.27929688, ((0, 64), (2, 4)))
    up_weight = scatter_about(arg_keys[10], (EXPERTS, D, FF), 0.046875, 0.27929688, ((0, 64), (2, 4)))
    down_weight = scatter_about(arg_keys[11], (EXPERTS, FF, D), (16 * FF) ** -0.5, 0.046875, ((0, 64), (1, 4)))
    return {"projected_queries": projected_queries, "key_proj": key_proj, "projected_values": projected_values, "head_sink_logits": head_sink_logits, "out_weight": out_weight, "expert_input": expert_input, "norm_gain": norm_gain, "routing": routing, "route_weight": route_weight, "gate_weight": gate_weight, "up_weight": up_weight, "down_weight": down_weight}


EPS = 1e-06
CLAMP = 7.0
SLOPE = 1.702

def attend_single_head(kernel_inputs, permitted_mask):
    query_head, key_head, value_head, sink_head = kernel_inputs
    scores = jnp.einsum('nqgd,nsd->ngqs', query_head, key_head) * HEAD_SIZE ** (-0.5)
    scores = jnp.where(permitted_mask[:, None, :, :], scores, -jnp.inf)
    sink_col = sink_head[None, :, None, None]
    highest = jnp.maximum(lax.optimization_barrier(jnp.max(scores, axis=-1, keepdims=True)), sink_col)
    numerator = jnp.exp(scores - highest)
    denominator = lax.optimization_barrier(jnp.sum(numerator, axis=-1, keepdims=True)) + jnp.exp(sink_col - highest)
    weights = (numerator / denominator).astype(jnp.bfloat16)
    return jnp.einsum('ngqs,nsd->nqgd', weights.astype(jnp.float32), value_head.astype(jnp.float32))

def slot_targets(flat_ids, capacity):
    onehot = (flat_ids[:, None] == jnp.arange(N_EP, dtype=jnp.int32)[None, :]).astype(jnp.int32)
    rank_in = jnp.cumsum(onehot, axis=0) - 1
    slot_pos = lax.optimization_barrier(jnp.sum(rank_in * onehot, axis=1))
    return (flat_ids * capacity + slot_pos).astype(jnp.int32)

def reference(projected_queries, key_proj, projected_values, head_sink_logits, out_weight, expert_input, norm_gain, routing, route_weight, gate_weight, up_weight, down_weight):
    total = projected_queries.shape[0]
    count_of_blocks = total // WINDOW_KEYS
    heads_per_group = QUERY_HEADS // KEY_VALUE_HEADS
    query_vectors = projected_queries.astype(jnp.float32).reshape(count_of_blocks, WINDOW_KEYS, KEY_VALUE_HEADS, heads_per_group, HEAD_SIZE)
    blank_rows = jnp.zeros((WINDOW_KEYS, KEY_VALUE_HEADS * HEAD_SIZE), jnp.bfloat16)
    padded_keys = jnp.concatenate([blank_rows, key_proj], axis=0).astype(jnp.float32)
    padded_values = jnp.concatenate([blank_rows, projected_values], axis=0)
    window_keys = jnp.concatenate([padded_keys[:-WINDOW_KEYS].reshape(count_of_blocks, WINDOW_KEYS, KEY_VALUE_HEADS, HEAD_SIZE), padded_keys[WINDOW_KEYS:].reshape(count_of_blocks, WINDOW_KEYS, KEY_VALUE_HEADS, HEAD_SIZE)], axis=1)
    window_values = jnp.concatenate([padded_values[:-WINDOW_KEYS].reshape(count_of_blocks, WINDOW_KEYS, KEY_VALUE_HEADS, HEAD_SIZE), padded_values[WINDOW_KEYS:].reshape(count_of_blocks, WINDOW_KEYS, KEY_VALUE_HEADS, HEAD_SIZE)], axis=1)
    block_ids = jnp.arange(count_of_blocks)[:, None, None] * WINDOW_KEYS
    query_pos = block_ids + jnp.arange(WINDOW_KEYS)[None, :, None] + WINDOW_KEYS
    key_pos = block_ids + jnp.arange(2 * WINDOW_KEYS)[None, None, :]
    permitted_mask = (key_pos <= query_pos) & (query_pos - key_pos < WINDOW_KEYS) & (key_pos >= WINDOW_KEYS)
    head_outputs = lax.map(lambda kernel_inputs: attend_single_head(kernel_inputs, permitted_mask), (query_vectors.transpose(2, 0, 1, 3, 4), window_keys.transpose(2, 0, 1, 3), window_values.transpose(2, 0, 1, 3), head_sink_logits.reshape(KEY_VALUE_HEADS, heads_per_group)))
    attended = head_outputs.transpose(1, 2, 0, 3, 4).reshape(total, QUERY_HEADS * HEAD_SIZE).astype(jnp.bfloat16)
    head_share = QUERY_HEADS * HEAD_SIZE // N_TP
    summed = jnp.zeros((total, D), jnp.float32)
    for group in range(N_TP):
        partial_value = jnp.dot(attended[:, group * head_share:(group + 1) * head_share], out_weight[group * head_share:(group + 1) * head_share], preferred_element_type=jnp.float32).astype(jnp.bfloat16)
        summed = summed + lax.optimization_barrier(partial_value).astype(jnp.float32)
    mixer_output = summed.astype(jnp.bfloat16)
    capacity = CAP
    widened = expert_input.astype(jnp.float32)
    normed = (widened * lax.rsqrt(lax.optimization_barrier(jnp.mean(widened * widened, axis=-1, keepdims=True)) + EPS) * norm_gain[None, :]).astype(jnp.bfloat16)
    per_source = TOK_B_DEV * TOPK
    flat_ids = routing.reshape(N_EP, per_source).astype(jnp.int32)
    target = jax.vmap(lambda id_row: slot_targets(id_row, capacity))(flat_ids)
    tok_ids = (jnp.arange(per_source) // TOPK).astype(jnp.int32)
    slot_tok = jax.vmap(lambda tgt_row: jnp.full((N_EP * capacity,), TOK_B_DEV, jnp.int32).at[tgt_row].set(tok_ids))(target)
    extended = jnp.concatenate([normed.reshape(N_EP, TOK_B_DEV, D), jnp.zeros((N_EP, 1, D), jnp.bfloat16)], axis=1)

    def run_expert(expert_id):
        picks = lax.dynamic_slice_in_dim(slot_tok, expert_id * capacity, capacity, 1)
        expert_rows = jax.vmap(lambda block_rows, pick_row: jnp.take(block_rows, pick_row, axis=0))(extended, picks)
        expert_rows = expert_rows.reshape(N_EP * capacity, D)
        gate_pre = jnp.dot(expert_rows, gate_weight[expert_id], preferred_element_type=jnp.float32)
        up_pre = jnp.dot(expert_rows, up_weight[expert_id], preferred_element_type=jnp.float32)
        gate_cut = jnp.minimum(gate_pre, CLAMP)
        activated = ((jnp.clip(up_pre, -CLAMP, CLAMP) + 1.0) * gate_cut * jax.nn.sigmoid(SLOPE * gate_cut)).astype(jnp.bfloat16)
        return jnp.dot(activated, down_weight[expert_id], preferred_element_type=jnp.float32).astype(jnp.bfloat16)
    results = lax.map(run_expert, jnp.arange(N_EP, dtype=jnp.int32))
    source = jnp.arange(N_EP, dtype=jnp.int32)[:, None]
    slot_of = target - flat_ids * capacity
    gather_at = ((flat_ids * N_EP + source) * capacity + slot_of).astype(jnp.int32)
    picked = jnp.take(results.reshape(-1, D), gather_at.reshape(-1), axis=0).astype(jnp.float32)
    picked = picked.reshape(N_EP * TOK_B_DEV, TOPK, D)
    expert_output = lax.optimization_barrier(jnp.sum(picked * route_weight[:, :, None], axis=1)).astype(jnp.bfloat16)
    return (mixer_output, expert_output)
```

```python
import jax
import jax.numpy as jnp
from jax import lax
from jax.experimental import pallas as pl
from jax.experimental.pallas import tpu as pltpu
from jax.sharding import PartitionSpec as P

EPS = 1e-06
CLAMP = 7.0
SLOPE = 1.702

NZ = 8
NQ = 8
NY = 4
D = 4096
TOK = 128
CAP = 12
ROWS = NZ * CAP
FC = 256
C = 8
HID = 256
NB = 4
MESH = pl.DeviceIdType.MESH
F32 = jnp.float32
BF16 = jnp.bfloat16


def kernel(
    q_ref, k_ref, v_ref, sink_ref, wo_hbm, x_ref, gain_ref, rt_ref, rw_ref, wg_hbm, wu_hbm, wd_hbm,
    mix_ref, out_ref,
    G, XS, XF, XO, WG, WU, WO, DN, S, CM, INFOS, IR, ACCG, ACCU, ACT, YS, RX, SR, RR,
    KP, KX, VX, ATT, PT, PM,
    ls, zss, zrs, iss, irs, xss, xrs, yss, yrs, dss, drs, ass, ars, wss, wrs, sss, srs, mss, mrs, hss, hrs,
):
    ep = lax.axis_index("ep")
    y = lax.axis_index("tp")
    z = ep // NQ
    q = lax.rem(ep, NQ)
    half = lax.rem(y, 2)

    def wrap(a, n):
        return lax.rem(a + n, n)

    def at_z(zz):
        return (zz * NQ + q, y)

    def at_q(qq):
        return (z * NQ + qq, y)

    def at_y(yy):
        return (ep, yy)

    def remote(src, dst, ss, rs, dev):
        return pltpu.make_async_remote_copy(src, dst, ss, rs, device_id=dev, device_id_type=MESH)

    barrier = pltpu.get_barrier_semaphore()
    next_ep, prev_ep = wrap(ep + 1, NZ * NQ), wrap(ep - 1, NZ * NQ)
    for i in range(1, NZ):
        pl.semaphore_signal(barrier, inc=1, device_id=at_z(wrap(z + i, NZ)), device_id_type=MESH)
    for i in range(1, NQ):
        pl.semaphore_signal(barrier, inc=1, device_id=at_q(wrap(q + i, NQ)), device_id_type=MESH)
    for i in range(1, NY):
        pl.semaphore_signal(barrier, inc=1, device_id=at_y(wrap(y + i, NY)), device_id_type=MESH)
    for e in (next_ep, prev_ep):
        pl.semaphore_signal(barrier, inc=1, device_id=(e, y), device_id_type=MESH)

    loads = [
        pltpu.make_async_copy(wg_hbm, WG, ls.at[0]),
        pltpu.make_async_copy(wu_hbm, WU, ls.at[1]),
        pltpu.make_async_copy(wo_hbm, WO, ls.at[2]),
        pltpu.make_async_copy(wd_hbm.at[:, pl.ds(pl.multiple_of(y * 1024, 1024), 1024)], DN.at[y], ls.at[3]),
    ]
    for load in loads:
        load.start()

    def mean_step(j, total):
        w = x_ref[:, pl.ds(pl.multiple_of(j * 512, 512), 512)].astype(F32)
        return total + jnp.sum(w * w, axis=1, keepdims=True)

    total = lax.fori_loop(0, D // 512, mean_step, jnp.zeros((TOK, 1), F32))
    scale = lax.rsqrt(total * (1.0 / D) + EPS)

    def norm_step(j, _):
        cols = pl.ds(pl.multiple_of(half * (C * FC) + j * FC, FC), FC)
        G[j, z] = (x_ref[:, cols].astype(F32) * scale * gain_ref[:, cols]).astype(BF16)
        return 0

    lax.fori_loop(0, C, norm_step, 0)

    lane = lax.broadcasted_iota(jnp.int32, (TOK, 128), 1)
    sub = lax.broadcasted_iota(jnp.int32, (TOK, 128), 0)
    expert = lane & 63
    named = jnp.zeros((TOK, 128), F32)
    weight = jnp.zeros((TOK, 128), F32)
    for k in range(4):
        hit = (rt_ref[:, k : k + 1] == expert).astype(F32)
        named = named + hit
        weight = weight + hit * rw_ref[:, k : k + 1]
    earlier = (lane < sub).astype(F32).astype(BF16)
    rank = jnp.dot(earlier, named.astype(BF16), preferred_element_type=F32)
    info = jnp.where(lane < 64, jnp.where(named > 0.5, rank, -1.0), weight).T
    INFOS[:, 0:8, :] = info[:64].reshape(NZ, 8, 128)
    INFOS[:, 8:16, :] = info[64:].reshape(NZ, 8, 128)
    IR[z] = INFOS[z]

    def z_copy(j, s, d):
        if d == 0:
            origin, peer = wrap(z - s, NZ), wrap(z + 1, NZ)
        else:
            origin, peer = wrap(z + s, NZ), wrap(z - 1, NZ)
        return remote(G.at[j, origin], G.at[j, origin], zss.at[d, s, j], zrs.at[d, s, j], at_z(peer))

    def i_copy(i):
        to = wrap(z + i, NZ)
        return remote(INFOS.at[to], IR.at[z], iss.at[i], irs.at[i], at_z(to))

    def x_copy(j, to):
        i = wrap(to - q, NQ)
        return remote(XS.at[j, to], XF.at[j, q], xss.at[j, i], xrs.at[j, i], at_q(to))

    def y_copy(j, d):
        to = wrap(y + 1, NY) if d == 0 else wrap(y - 1, NY)
        part = pl.ds(4 * d, 4)
        return remote(XF.at[j, part], XO.at[j, part], yss.at[d, j], yrs.at[d, j], at_y(to))

    def d_copy(i):
        to = wrap(y + i, NY)
        src = wd_hbm.at[:, pl.ds(pl.multiple_of(to * 1024, 1024), 1024)]
        return remote(src, DN.at[y], dss.at[i], drs.at[i], at_y(to))

    def a_copy(r, i):
        to = wrap(y + i, NY)
        part = pl.ds(2 * r, 2)
        return remote(ACT.at[y, part], ACT.at[y, part], ass.at[i, r], ars.at[i, r], at_y(to))

    def w_copy(n, to):
        i = wrap(to - q, NQ)
        return remote(YS.at[n, to], RX.at[n, q], wss.at[n, i], wrs.at[n, i], at_q(to))

    def s_copy(n, s, d):
        peer = wrap(z + 1, NZ) if d == 0 else wrap(z - 1, NZ)
        return remote(SR.at[d, n, s], RR.at[d, n, s], sss.at[d, n, s], srs.at[d, n, s], at_z(peer))

    def m_copy(i):
        to = wrap(y + i, NY)
        return remote(PT.at[to], PM.at[i], mss.at[i], mrs.at[i], at_y(to))

    halo = [
        remote(k_ref.at[pl.ds(128, 128)], KP.at[0], hss.at[0], hrs.at[0], (next_ep, y)),
        remote(v_ref.at[pl.ds(128, 128)], KP.at[1], hss.at[1], hrs.at[1], (next_ep, y)),
    ]

    pl.semaphore_wait(barrier, (NZ - 1) + (NQ - 1) + (NY - 1) + 2)
    for d in range(2):
        z_copy(0, 0, d).start()
    for i in range(1, NZ):
        i_copy(i).start()
    for copy in halo:
        copy.start()
    for i in (2, 1, 3):
        d_copy(i).start()
    ACCG[...] = jnp.zeros_like(ACCG)
    ACCU[...] = jnp.zeros_like(ACCU)

    def build_windows():
        for copy in halo:
            copy.wait_recv()
        lanes = lax.broadcasted_iota(jnp.int32, (384, 128), 1)
        for t, (ref, wide) in enumerate(((k_ref, KX), (v_ref, VX))):
            whole = jnp.concatenate([KP[t], ref[...]], axis=0).astype(F32)
            turned = pltpu.roll(whole, 64, 1)
            zero = jnp.zeros_like(whole)
            wide[0, 0] = jnp.where(lanes < 64, whole, zero).astype(BF16)
            wide[1, 1] = jnp.where(lanes < 64, zero, whole).astype(BF16)
            wide[0, 1] = jnp.where(lanes < 64, zero, turned).astype(BF16)
            wide[1, 0] = jnp.where(lanes < 64, turned, zero).astype(BF16)

    def div12(a):
        return (a * 5462) >> 16

    def build_gather():
        for i in range(1, NZ):
            i_copy(i).wait_recv()
        row = lax.broadcasted_iota(jnp.int32, (ROWS, 128), 0)
        row_z = div12(row)
        row_k = (row - row_z * CAP).astype(F32)

        def step(zs, _):
            cols = pl.ds(pl.multiple_of(zs * TOK, TOK), TOK)
            ranks = IR[zs, 0:8, :]
            for e in range(NQ):
                hit = (row_z == zs) & (ranks[e : e + 1, :] == row_k)
                S[e, :, cols] = hit.astype(F32).astype(BF16)
            return 0

        lax.fori_loop(0, NZ, step, 0)

    def build_combine():
        i16 = lax.broadcasted_iota(jnp.int32, (16, NQ * ROWS), 0)
        col = lax.broadcasted_iota(jnp.int32, (16, NQ * ROWS), 1)
        col_q = (div12(col)) >> 3
        spread_rank = (i16 == col_q).astype(F32).astype(BF16)
        spread_weight = (i16 == col_q + 8).astype(F32).astype(BF16)
        col = lax.broadcasted_iota(jnp.int32, (TOK, NQ * ROWS), 1)
        col12 = div12(col)
        col_z = col12 & 7
        col_k = (col - col12 * CAP).astype(F32)

        def step(zs, _):
            turned = IR[zs].T.astype(BF16)
            ranks = jnp.dot(turned, spread_rank, preferred_element_type=F32)
            weights = jnp.dot(turned, spread_weight, preferred_element_type=F32)
            hit = (col_z == zs) & (ranks == col_k)
            CM[zs] = jnp.where(hit, weights, 0.0).astype(BF16)
            return 0

        lax.fori_loop(0, NZ, step, 0)

    def attend(u):
        n, p = u // 4, lax.rem(u, 4)
        kv = p // 2
        rows = pl.ds(pl.multiple_of(n * 128, 128), 128)
        window = pl.ds(pl.multiple_of(n * 128, 128), 256)
        cols = pl.ds(pl.multiple_of(p * 128, 128), 128)
        queries = q_ref[rows, cols]
        i = lax.broadcasted_iota(jnp.int32, (128, 256), 0)
        s = lax.broadcasted_iota(jnp.int32, (128, 256), 1)
        first = jnp.where((ep == 0) & (n == 0), 128, 0)
        seen = (s > i) & (s <= i + 128) & (s >= first)
        both = jnp.zeros((128, 128), F32)
        for h in range(2):
            scores = lax.dot_general(
                queries, KX[kv, h, window, :], (((1,), (1,)), ((), ())), preferred_element_type=F32
            ) * 0.125
            scores = jnp.where(seen, scores, -jnp.inf)
            sink = sink_ref[2 * p + h]
            highest = jnp.maximum(jnp.max(scores, axis=1, keepdims=True), sink)
            e = jnp.exp(scores - highest)
            under = jnp.sum(e, axis=1, keepdims=True) + jnp.exp(sink - highest)
            w = (e / under).astype(BF16)
            both = both + jnp.dot(w, VX[kv, h, window, :], preferred_element_type=F32)
        ATT[rows, cols] = both.astype(BF16)

    def project(u):
        cols = pl.ds(pl.multiple_of(u * 512, 512), 512)
        part = jnp.dot(ATT[...], WO[:, cols], preferred_element_type=F32).astype(BF16)
        PT[:, :, cols] = part.reshape(NY, 64, 512)

    def expert_dots(src, j, w):
        def step(r, _):
            part = pl.ds(4 * r, 4)
            block = src[j, part].reshape(4 * ROWS, FC)
            rows = pl.ds(pl.multiple_of(r * 4 * ROWS, 4 * ROWS), 4 * ROWS)
            ACCG[rows, :] += jnp.dot(block, WG[w], preferred_element_type=F32)
            ACCU[rows, :] += jnp.dot(block, WU[w], preferred_element_type=F32)
            return 0

        lax.fori_loop(0, 2, step, 0)

    def within(j):
        return (j >= 0) & (j < C)

    def tick(t, _):
        @pl.when(t + 1 < C)
        def _():
            for d in range(2):
                z_copy(t + 1, 0, d).start()

        @pl.when(within(t - 3))
        def _():
            j = t - 3
            for d in range(2):
                z_copy(j, 2, d).wait_recv()

                @pl.when(lax.rem(j, 2) == d)
                def _():
                    z_copy(j, 3, d).start()

        for s in (2, 1):

            @pl.when(within(t - s))
            def _():
                for d in range(2):
                    z_copy(t - s, s - 1, d).wait_recv()
                    z_copy(t - s, s, d).start()

        @pl.when(within(t - 4))
        def _():
            j = t - 4
            for d in range(2):

                @pl.when(lax.rem(j, 2) == d)
                def _():
                    z_copy(j, 3, d).wait_recv()

            def step(r, _):
                part = pl.ds(4 * r, 4)
                block = jnp.dot(
                    S[part].reshape(4 * ROWS, NZ * TOK), G[j].reshape(NZ * TOK, FC), preferred_element_type=F32
                ).astype(BF16)
                XS[j, part] = block.reshape(4, ROWS, FC)
                for i in range(4):

                    @pl.when(4 * r + i != q)
                    def _():
                        x_copy(j, 4 * r + i).start()

                return 0

            lax.fori_loop(0, 2, step, 0)
            XF[j, q] = XS[j, q]

        @pl.when(within(t - 6))
        def _():
            j = t - 6
            for i in range(1, NQ):
                x_copy(j, wrap(q + i, NQ)).wait_recv()
            for d in range(2):
                y_copy(j, d).start()
            @pl.when(j == 0)
            def _():
                loads[0].wait()
                loads[1].wait()
            expert_dots(XF, j, half * C + j)

        @pl.when(within(t - 8))
        def _():
            j = t - 8
            for d in range(2):
                y_copy(j, d).wait_recv()
            expert_dots(XO, j, (1 - half) * C + j)

        @pl.when(t == 0)
        def _():
            build_windows()

        @pl.when(t == 1)
        def _():
            build_gather()

        @pl.when((t >= 2) & (t < 6))
        def _():
            for i in range(2):
                attend((t - 2) * 2 + i)

        @pl.when(t == 6)
        def _():
            loads[2].wait()

        @pl.when((t >= 6) & (t < 10))
        def _():
            for i in range(2):
                project((t - 6) * 2 + i)

        @pl.when(t == 10)
        def _():
            build_combine()

        return 0

    lax.fori_loop(0, C + 8, tick, 0)

    def activate(r, _):
        rows = pl.ds(pl.multiple_of(r * 2 * ROWS, 2 * ROWS), 2 * ROWS)
        g = jnp.minimum(ACCG[rows, :], CLAMP)
        u = jnp.clip(ACCU[rows, :], -CLAMP, CLAMP) + 1.0
        a = (u * g * jax.nn.sigmoid(SLOPE * g)).astype(BF16)
        ACT[y, pl.ds(2 * r, 2)] = a.reshape(2, ROWS, HID)
        for i in (2, 1, 3):
            a_copy(r, i).start()
        return 0

    lax.fori_loop(0, 4, activate, 0)
    for i in (2, 1, 3):
        m_copy(i).start()
    loads[3].wait()
    for i in range(1, NY):
        d_copy(i).wait_recv()

    def arrive(r, _):
        for i in range(1, NY):
            a_copy(r, i).wait_recv()
        return 0

    lax.fori_loop(0, 4, arrive, 0)

    def down(n, _):
        cols = pl.ds(pl.multiple_of(n * FC, FC), FC)

        def step(r, _):
            part = pl.ds(4 * r, 4)
            block = jnp.dot(ACT[0, part].reshape(4 * ROWS, HID), DN[0, :, cols], preferred_element_type=F32)
            for i in range(1, NY):
                block = block + jnp.dot(
                    ACT[i, part].reshape(4 * ROWS, HID), DN[i, :, cols], preferred_element_type=F32
                )
            YS[n, part] = block.astype(BF16).reshape(4, ROWS, FC)
            for i in range(4):

                @pl.when(4 * r + i != q)
                def _():
                    w_copy(n, 4 * r + i).start()

            return 0

        lax.fori_loop(0, 2, step, 0)
        RX[n, q] = YS[n, q]
        return 0

    lax.fori_loop(0, NB, down, 0)

    def partial_sum(n, zd):
        return jnp.dot(CM[zd], RX[n].reshape(NQ * ROWS, FC), preferred_element_type=F32)

    def send_sum(n, s, d):
        odd = lax.rem(n, 2)
        ahead = (4 - odd if d == 0 else 3 + odd) - s
        zd = wrap(z + ahead, NZ) if d == 0 else wrap(z - ahead, NZ)
        value = partial_sum(n, zd)
        if s > 0:
            s_copy(n, s - 1, d).wait_recv()
            value = value + RR[d, n, s - 1].astype(F32)
        SR[d, n, s] = value.astype(BF16)
        s_copy(n, s, d).start()

    def wave(w, _):
        for s in (3, 2, 1, 0):
            n = w - s

            @pl.when((n >= 0) & (n < NB))
            def _():
                if s == 0:
                    for i in range(1, NQ):
                        w_copy(n, wrap(q + i, NQ)).wait_recv()
                for d in range(2):
                    if s < 3:
                        send_sum(n, s, d)
                    else:

                        @pl.when(lax.rem(n, 2) == d)
                        def _():
                            send_sum(n, s, d)

        @pl.when((w - 4 >= 0) & (w - 4 < NB))
        def _():
            n = w - 4
            odd = lax.rem(n, 2)
            value = partial_sum(n, z)
            for d in range(2):
                last = 3 - odd if d == 0 else 2 + odd
                s_copy(n, last, d).wait_recv()
                value = value + RR[d, n, last].astype(F32)
            out_ref[:, pl.ds(pl.multiple_of(n * FC, FC), FC)] = value.astype(BF16)

        return 0

    lax.fori_loop(0, NB + 4, wave, 0)

    for i in range(1, NY):
        m_copy(i).wait_recv()

    def mix(u, _):
        cols = pl.ds(pl.multiple_of(u * 512, 512), 512)
        value = PT[y, :, cols].astype(F32)
        for i in range(1, NY):
            value = value + PM[i, :, cols].astype(F32)
        mix_ref[:, cols] = value.astype(BF16)
        return 0

    lax.fori_loop(0, D // 512, mix, 0)

    def sent_chunk(j, _):
        for d in range(2):
            for s in range(3):
                z_copy(j, s, d).wait_send()

            @pl.when(lax.rem(j, 2) == d)
            def _():
                z_copy(j, 3, d).wait_send()

            y_copy(j, d).wait_send()
        for i in range(1, NQ):
            x_copy(j, wrap(q + i, NQ)).wait_send()
        return 0

    lax.fori_loop(0, C, sent_chunk, 0)

    def sent_block(n, _):
        for d in range(2):
            for s in range(3):
                s_copy(n, s, d).wait_send()

            @pl.when(lax.rem(n, 2) == d)
            def _():
                s_copy(n, 3, d).wait_send()

        for i in range(1, NQ):
            w_copy(n, wrap(q + i, NQ)).wait_send()
        for i in range(1, NY):
            a_copy(n, i).wait_send()
        return 0

    lax.fori_loop(0, NB, sent_block, 0)
    for i in range(1, NZ):
        i_copy(i).wait_send()
    for i in range(1, NY):
        d_copy(i).wait_send()
        m_copy(i).wait_send()
    for copy in halo:
        copy.wait_send()


def shards(
    projected_queries,
    key_proj,
    projected_values,
    head_sink_logits,
    out_weight,
    expert_input,
    norm_gain,
    routing,
    route_weight,
    gate_weight,
    up_weight,
    down_weight,
):
    vmem = pl.BlockSpec(memory_space=pltpu.VMEM)
    hbm = pl.BlockSpec(memory_space=pl.ANY)
    smem = pl.BlockSpec(memory_space=pltpu.SMEM)
    dma = pltpu.SemaphoreType.DMA
    return pl.pallas_call(
        kernel,
        out_shape=(
            jax.ShapeDtypeStruct((64, D), BF16),
            jax.ShapeDtypeStruct((TOK, 1024), BF16),
        ),
        in_specs=[vmem, vmem, vmem, smem, hbm, vmem, vmem, vmem, vmem, hbm, hbm, hbm],
        out_specs=(vmem, vmem),
        scratch_shapes=[
            pltpu.VMEM((C, NZ, TOK, FC), BF16),
            pltpu.VMEM((C, NQ, ROWS, FC), BF16),
            pltpu.VMEM((C, NQ, ROWS, FC), BF16),
            pltpu.VMEM((C, NQ, ROWS, FC), BF16),
            pltpu.VMEM((2 * C, FC, HID), BF16),
            pltpu.VMEM((2 * C, FC, HID), BF16),
            pltpu.VMEM((512, D), BF16),
            pltpu.VMEM((NY, HID, 1024), BF16),
            pltpu.VMEM((NQ, ROWS, NZ * TOK), BF16),
            pltpu.VMEM((NZ, TOK, NQ * ROWS), BF16),
            pltpu.VMEM((NZ, 16, 128), F32),
            pltpu.VMEM((NZ, 16, 128), F32),
            pltpu.VMEM((NQ * ROWS, HID), F32),
            pltpu.VMEM((NQ * ROWS, HID), F32),
            pltpu.VMEM((NY, NQ, ROWS, HID), BF16),
            pltpu.VMEM((NB, NQ, ROWS, FC), BF16),
            pltpu.VMEM((NB, NQ, ROWS, FC), BF16),
            pltpu.VMEM((2, NB, 4, TOK, FC), BF16),
            pltpu.VMEM((2, NB, 4, TOK, FC), BF16),
            pltpu.VMEM((2, 128, 128), BF16),
            pltpu.VMEM((2, 2, 384, 128), BF16),
            pltpu.VMEM((2, 2, 384, 128), BF16),
            pltpu.VMEM((256, 512), BF16),
            pltpu.VMEM((NY, 64, D), BF16),
            pltpu.VMEM((NY, 64, D), BF16),
            dma((4,)),
            dma((2, 4, C)), dma((2, 4, C)),
            dma((NZ,)), dma((NZ,)),
            dma((C, NQ)), dma((C, NQ)),
            dma((2, C)), dma((2, C)),
            dma((NY,)), dma((NY,)),
            dma((NY, 4)), dma((NY, 4)),
            dma((NB, NQ)), dma((NB, NQ)),
            dma((2, NB, 4)), dma((2, NB, 4)),
            dma((NY,)), dma((NY,)),
            dma((2,)), dma((2,)),
        ],
        compiler_params=pltpu.CompilerParams(
            collective_id=0, has_side_effects=True, vmem_limit_bytes=62 * 1024 * 1024
        ),
    )(
        projected_queries,
        key_proj,
        projected_values,
        head_sink_logits,
        out_weight,
        expert_input,
        norm_gain.reshape(1, D),
        routing,
        route_weight,
        gate_weight.reshape(2 * C, FC, HID),
        up_weight.reshape(2 * C, FC, HID),
        down_weight.reshape(HID, D),
    )


def solution(mesh):
    placed = (
        P("ep", "tp"),
        P("ep", "tp"),
        P("ep", "tp"),
        P("tp"),
        P("tp", None),
        P("ep", None),
        P(),
        P("ep", None),
        P("ep", None),
        P("ep", None, "tp"),
        P("ep", None, "tp"),
        P("ep", "tp", None),
    )
    return jax.shard_map(
        shards,
        mesh=mesh,
        in_specs=placed,
        out_specs=(P(("ep", "tp"), None), P("ep", "tp")),
        check_vma=False,
    )
```

```python
import jax
import jax.numpy as jnp
from jax import lax
from jax.experimental import pallas as pl
from jax.experimental.pallas import tpu as pltpu
from jax.sharding import PartitionSpec as P

EPS = 1e-06
CLAMP = 7.0
SLOPE = 1.702

NZ = 8
NQ = 8
NY = 4
D = 4096
TOK = 128
CAP = 12
ROWS = NZ * CAP
FC = 256
CE = 7
C = 9
AHEAD = 2
HID = 256
NB = 4
MESH = pl.DeviceIdType.MESH
F32 = jnp.float32
BF16 = jnp.bfloat16


def kernel(
    q_hbm, k_hbm, v_hbm, sink_ref, wo_hbm, x_hbm, gain_hbm, rt_hbm, rw_hbm, wg_hbm, wu_hbm, wd_hbm,
    mix_ref, out_ref,
    q_ref, k_ref, v_ref, x_ref, gain_ref, rt_ref, rw_ref,
    G, XS, XF, XO, W, WO, DN, S, CM, IR, RANK, ACC, ACT, YS, RX, SR, RR,
    KP, KX, VX, ATT, PT, PM,
    ls, zss, zrs, iss, irs, xss, xrs, yss, yrs, dss, drs, ass, ars, wss, wrs, sss, srs, mss, mrs, hss, hrs,
):
    ep = lax.axis_index("ep")
    y = lax.axis_index("tp")
    z = ep // NQ
    q = lax.rem(ep, NQ)
    half = lax.rem(y, 2)

    def wrap(a, n):
        return lax.rem(a + n, n)

    def at_z(zz):
        return (zz * NQ + q, y)

    def at_q(qq):
        return (z * NQ + qq, y)

    def at_y(yy):
        return (ep, yy)

    def remote(src, dst, ss, rs, dev):
        return pltpu.make_async_remote_copy(src, dst, ss, rs, device_id=dev, device_id_type=MESH)

    barrier = pltpu.get_barrier_semaphore()
    next_ep, prev_ep = wrap(ep + 1, NZ * NQ), wrap(ep - 1, NZ * NQ)
    for i in (1, NZ - 1):
        pl.semaphore_signal(barrier, inc=1, device_id=at_z(wrap(z + i, NZ)), device_id_type=MESH)
    for i in range(1, NQ):
        pl.semaphore_signal(barrier, inc=1, device_id=at_q(wrap(q + i, NQ)), device_id_type=MESH)
    for i in range(1, NY):
        pl.semaphore_signal(barrier, inc=1, device_id=at_y(wrap(y + i, NY)), device_id_type=MESH)
    for e in (next_ep, prev_ep):
        pl.semaphore_signal(barrier, inc=1, device_id=(e, y), device_id_type=MESH)

    own_down = wd_hbm.at[:, pl.ds(pl.multiple_of(y * 1024, 1024), 1024)]
    pairs = (
        (x_hbm, x_ref), (gain_hbm, gain_ref), (rt_hbm, rt_ref), (rw_hbm, rw_ref),
        (k_hbm, k_ref), (v_hbm, v_ref), (q_hbm, q_ref),
        (wg_hbm, W.at[:, :, pl.ds(0, HID)]), (wu_hbm, W.at[:, :, pl.ds(HID, HID)]), (wo_hbm, WO), (own_down, DN.at[y]),
    )
    loads = [pltpu.make_async_copy(src, dst, ls.at[i]) for i, (src, dst) in enumerate(pairs)]
    for load in loads:
        load.start()

    def chunk(j):
        return jnp.where(j < CE, half * CE + j, CE + j)

    loads[0].wait()

    def mean_step(j, total):
        w = x_ref[:, pl.ds(pl.multiple_of(j * 512, 512), 512)].astype(F32)
        return total + jnp.sum(w * w, axis=1, keepdims=True)

    total = lax.fori_loop(0, D // 512, mean_step, jnp.zeros((TOK, 1), F32))
    scale = lax.rsqrt(total * (1.0 / D) + EPS)
    for i in (1, 2, 3):
        loads[i].wait()

    def norm_step(j, _):
        cols = pl.ds(pl.multiple_of(chunk(j) * FC, FC), FC)
        G[j, z] = (x_ref[:, cols].astype(F32) * scale * gain_ref[:, cols]).astype(BF16)
        return 0

    lax.fori_loop(0, C, norm_step, 0)
    IR[z] = jnp.concatenate([rt_ref[...].astype(F32), rw_ref[...]], axis=0)

    def hop(s, d):
        return 6 if s == 3 else 2 * s + d

    def z_copy(j, s, d):
        if d == 0:
            origin, peer = wrap(z - s, NZ), wrap(z + 1, NZ)
        else:
            origin, peer = wrap(z + s, NZ), wrap(z - 1, NZ)
        return remote(G.at[j, origin], G.at[j, origin], zss.at[0], zrs.at[j, hop(s, d)], at_z(peer))

    def i_copy(s, d):
        if d == 0:
            origin, peer = wrap(z - s, NZ), wrap(z + 1, NZ)
        else:
            origin, peer = wrap(z + s, NZ), wrap(z - 1, NZ)
        return remote(IR.at[origin], IR.at[origin], iss.at[0], irs.at[hop(s, d)], at_z(peer))

    def x_copy(j, to):
        return remote(XS.at[j, to], XF.at[j, q], xss.at[0], xrs.at[j], at_q(to))

    def y_copy(j, d):
        to = wrap(y + 1, NY) if d == 0 else wrap(y - 1, NY)
        part = pl.ds(4 * d, 4)
        return remote(XF.at[j, part], XO.at[j, part], yss.at[0], yrs.at[j], at_y(to))

    def d_copy(i):
        to = wrap(y + i, NY)
        src = wd_hbm.at[:, pl.ds(pl.multiple_of(to * 1024, 1024), 1024)]
        return remote(src, DN.at[y], dss.at[0], drs.at[0], at_y(to))

    def a_copy(qq, b, i):
        to = wrap(y + i, NY)
        return remote(ACT.at[y, qq], ACT.at[y, qq], ass.at[0], ars.at[b], at_y(to))

    def w_copy(to):
        return remote(YS.at[to], RX.at[q], wss.at[0], wrs.at[0], at_q(to))

    def s_copy(n, h, d):
        peer = wrap(z + 1, NZ) if d == 0 else wrap(z - 1, NZ)
        return remote(SR.at[n, h], RR.at[n, h], sss.at[0], srs.at[n, h], at_z(peer))

    def m_copy(i):
        to = wrap(y + i, NY)
        return remote(PT.at[to], PM.at[i], mss.at[0], mrs.at[0], at_y(to))

    halo = [
        remote(k_hbm.at[pl.ds(128, 128)], KP.at[0], hss.at[0], hrs.at[0], (next_ep, y)),
        remote(v_hbm.at[pl.ds(128, 128)], KP.at[1], hss.at[0], hrs.at[0], (next_ep, y)),
    ]

    def wait_bytes(view, sem):
        pltpu.make_async_copy(view, view, sem).wait()

    pl.semaphore_wait(barrier, 2 + (NQ - 1) + (NY - 1) + 2)
    for d in range(2):
        z_copy(0, 0, d).start()
        i_copy(0, d).start()
    for j in range(1, AHEAD):
        for d in range(2):
            z_copy(j, 0, d).start()
    for copy in halo:
        copy.start()
    for i in (2, 1, 3):
        d_copy(i).start()
    ACC[...] = jnp.zeros_like(ACC)

    def build_windows():
        wait_bytes(KP, hrs.at[0])
        for i in (4, 5, 6):
            loads[i].wait()
        lanes = lax.broadcasted_iota(jnp.int32, (384, 128), 1)
        for t, (ref, wide) in enumerate(((k_ref, KX), (v_ref, VX))):
            whole = jnp.concatenate([KP[t], ref[...]], axis=0).astype(F32)
            turned = pltpu.roll(whole, 64, 1)
            zero = jnp.zeros_like(whole)
            wide[0, 0] = jnp.where(lanes < 64, whole, zero).astype(BF16)
            wide[1, 1] = jnp.where(lanes < 64, zero, whole).astype(BF16)
            wide[0, 1] = jnp.where(lanes < 64, zero, turned).astype(BF16)
            wide[1, 0] = jnp.where(lanes < 64, turned, zero).astype(BF16)

    def div12(a):
        return (a * 5462) >> 16

    def build_gather():
        u = lax.broadcasted_iota(jnp.int32, (TOK, TOK), 0)
        t = lax.broadcasted_iota(jnp.int32, (TOK, TOK), 1)
        earlier = (u < t).astype(F32).astype(BF16)
        expert = (lax.broadcasted_iota(jnp.int32, (NQ, TOK), 0) + z * NQ).astype(F32)
        named, weight = [], []
        for zs in range(NZ):
            info = IR[zs]
            hits = [(info[k : k + 1, :] == expert).astype(F32) for k in range(4)]
            named.append(hits[0] + hits[1] + hits[2] + hits[3])
            weight.append(sum(hits[k] * info[4 + k : 5 + k, :] for k in range(4)))
        named = jnp.concatenate(named, axis=0)
        rank = jnp.dot(named.astype(BF16), earlier, preferred_element_type=F32)
        rank = jnp.where(named > 0.5, rank, -1.0)
        for zs in range(NZ):
            RANK[zs, 0:8, :] = rank[8 * zs : 8 * zs + 8, :]
            RANK[zs, 8:16, :] = weight[zs]
        row = lax.broadcasted_iota(jnp.int32, (ROWS, 128), 0)
        row_z = div12(row)
        row_k = (row - row_z * CAP).astype(F32)

        def step(zs, _):
            cols = pl.ds(pl.multiple_of(zs * TOK, TOK), TOK)
            ranks = RANK[zs, 0:8, :]
            for e in range(NQ):
                hit = (row_z == zs) & (ranks[e : e + 1, :] == row_k)
                S[e, :, cols] = hit.astype(F32).astype(BF16)
            return 0

        lax.fori_loop(0, NZ, step, 0)

    def build_combine():
        i16 = lax.broadcasted_iota(jnp.int32, (16, NQ * ROWS), 0)
        col = lax.broadcasted_iota(jnp.int32, (16, NQ * ROWS), 1)
        col_q = (div12(col)) >> 3
        spread_rank = (i16 == col_q).astype(F32).astype(BF16)
        spread_weight = (i16 == col_q + 8).astype(F32).astype(BF16)
        col = lax.broadcasted_iota(jnp.int32, (TOK, NQ * ROWS), 1)
        col12 = div12(col)
        col_z = col12 & 7
        col_k = (col - col12 * CAP).astype(F32)

        def step(zs, _):
            turned = RANK[zs].T.astype(BF16)
            ranks = jnp.dot(turned, spread_rank, preferred_element_type=F32)
            weights = jnp.dot(turned, spread_weight, preferred_element_type=F32)
            hit = (col_z == zs) & (ranks == col_k)
            CM[zs] = jnp.where(hit, weights, 0.0).astype(BF16)
            return 0

        lax.fori_loop(0, NZ, step, 0)

    def attend(u):
        n, p = u // 4, lax.rem(u, 4)
        kv = p // 2
        rows = pl.ds(pl.multiple_of(n * 128, 128), 128)
        window = pl.ds(pl.multiple_of(n * 128, 128), 256)
        cols = pl.ds(pl.multiple_of(p * 128, 128), 128)
        queries = q_ref[rows, cols]
        i = lax.broadcasted_iota(jnp.int32, (128, 256), 0)
        s = lax.broadcasted_iota(jnp.int32, (128, 256), 1)
        first = jnp.where((ep == 0) & (n == 0), 128, 0)
        seen = (s > i) & (s <= i + 128) & (s >= first)
        both = jnp.zeros((128, 128), F32)
        for h in range(2):
            scores = lax.dot_general(
                queries, KX[kv, h, window, :], (((1,), (1,)), ((), ())), preferred_element_type=F32
            ) * 0.125
            scores = jnp.where(seen, scores, -jnp.inf)
            sink = sink_ref[2 * p + h]
            highest = jnp.maximum(jnp.max(scores, axis=1, keepdims=True), sink)
            e = jnp.exp(scores - highest)
            under = jnp.sum(e, axis=1, keepdims=True) + jnp.exp(sink - highest)
            w = (e / under).astype(BF16)
            both = both + jnp.dot(w, VX[kv, h, window, :], preferred_element_type=F32)
        ATT[rows, cols] = both.astype(BF16)

    def project(u):
        cols = pl.ds(pl.multiple_of(u * 512, 512), 512)
        part = jnp.dot(ATT[...], WO[:, cols], preferred_element_type=F32).astype(BF16)
        PT[:, :, cols] = part.reshape(NY, 64, 512)

    def expert_dots(*terms):
        def step(r, _):
            part = pl.ds(4 * r, 4)
            rows = pl.ds(pl.multiple_of(r * 4 * ROWS, 4 * ROWS), 4 * ROWS)
            value = ACC[rows, :]
            for src, j, w in terms:
                block = src[j, part].reshape(4 * ROWS, FC)
                value = value + jnp.dot(block, W[w], preferred_element_type=F32)
            ACC[rows, :] = value
            return 0

        lax.fori_loop(0, 2, step, 0)

    def within(j):
        return (j >= 0) & (j < C)

    def tick(t, _):
        @pl.when(within(t - 3))
        def _():
            j = t - 3

            @pl.when(j == 0)
            def _():
                i_copy(2, 0).wait_recv()
                i_copy(2, 1).wait_recv()
                i_copy(3, 0).start()

            for d in range(2):
                z_copy(j, 2, d).wait_recv()

                @pl.when(lax.rem(j, 2) == d)
                def _():
                    z_copy(j, 3, d).start()

        for s in (2, 1):

            @pl.when(within(t - s))
            def _():
                for d in range(2):

                    @pl.when(t == s)
                    def _():
                        i_copy(s - 1, d).wait_recv()
                        i_copy(s, d).start()

                    z_copy(t - s, s - 1, d).wait_recv()
                    z_copy(t - s, s, d).start()

        @pl.when(t + AHEAD < C)
        def _():
            for d in range(2):
                z_copy(t + AHEAD, 0, d).start()

        @pl.when(within(t - 4))
        def _():
            j = t - 4

            @pl.when(j == 0)
            def _():
                i_copy(3, 0).wait_recv()
                build_gather()

            for d in range(2):

                @pl.when(lax.rem(j, 2) == d)
                def _():
                    z_copy(j, 3, d).wait_recv()

            def step(r, _):
                part = pl.ds(4 * r, 4)
                block = jnp.dot(
                    S[part].reshape(4 * ROWS, NZ * TOK), G[j].reshape(NZ * TOK, FC), preferred_element_type=F32
                ).astype(BF16)
                XS[j, part] = block.reshape(4, ROWS, FC)
                for i in range(4):

                    @pl.when(4 * r + i != q)
                    def _():
                        x_copy(j, 4 * r + i).start()

                return 0

            lax.fori_loop(0, 2, step, 0)
            XF[j, q] = XS[j, q]

        @pl.when(within(t - 6))
        def _():
            j = t - 6
            wait_bytes(XF.at[j, pl.ds(0, NQ - 1)], xrs.at[j])

            @pl.when(j < CE)
            def _():
                for d in range(2):
                    y_copy(j, d).start()

            @pl.when(j == 0)
            def _():
                loads[7].wait()
                loads[8].wait()

        @pl.when((t >= 6) & (t < 8))
        def _():
            expert_dots((XF, t - 6, chunk(t - 6)))

        @pl.when((t >= 8) & (t < 8 + CE))
        def _():
            j = t - 8
            wait_bytes(XO.at[j], yrs.at[j])
            expert_dots((XF, t - 6, chunk(t - 6)), (XO, j, (1 - half) * CE + j))

        @pl.when(t == 2)
        def _():
            build_windows()

        @pl.when((t >= 3) & (t < 7))
        def _():
            for i in range(2):
                attend((t - 3) * 2 + i)

        return 0

    lax.fori_loop(0, C + 6, tick, 0)

    def pair(b):
        chip, core = q // 2, lax.rem(q, 2)
        apart = (b > 0) & (b < 3)
        dx = jnp.where(b == 0, 2, jnp.where(b == 3, 0, 1))
        dc = jnp.where(apart, b - 1, 0)
        first = lax.rem(chip + dx, 4) * 2 + lax.rem(core + dc, 2)
        dx = jnp.where(apart, 3, dx)
        dc = jnp.where(apart, b - 1, 1)
        return first, lax.rem(chip + dx, 4) * 2 + lax.rem(core + dc, 2)

    def activate(b, _):
        for qq in pair(b):
            rows = pl.ds(pl.multiple_of(qq * ROWS, ROWS), ROWS)
            g = jnp.minimum(ACC[rows, 0:HID], CLAMP)
            u = jnp.clip(ACC[rows, HID : 2 * HID], -CLAMP, CLAMP) + 1.0
            ACT[y, qq] = (u * g * jax.nn.sigmoid(SLOPE * g)).astype(BF16)
            for i in (2, 1, 3):
                a_copy(qq, b, i).start()
        return 0

    lax.fori_loop(0, 4, activate, 0)
    build_combine()
    loads[9].wait()

    def project_step(u, _):
        project(u)
        return 0

    lax.fori_loop(0, D // 512, project_step, 0)
    loads[10].wait()
    wait_bytes(DN.at[pl.ds(0, NY - 1)], drs.at[0])

    def down(b, _):
        wait_bytes(ACT.at[pl.ds(0, NY - 1), pl.ds(0, 2)], ars.at[b])

        @pl.when(b == 3)
        def _():
            for i in (2, 1, 3):
                m_copy(i).start()

        qs = pair(b)
        block = jnp.zeros((2 * ROWS, 1024), F32)
        for i in range(NY):
            acts = jnp.concatenate([ACT[i, qq] for qq in qs], axis=0)
            block = block + jnp.dot(acts, DN[i], preferred_element_type=F32)
        for i, qq in enumerate(qs):
            YS[qq] = block[i * ROWS : (i + 1) * ROWS].astype(BF16)

            @pl.when(qq != q)
            def _():
                w_copy(qq).start()

        return 0

    lax.fori_loop(0, 4, down, 0)
    RX[q] = YS[q]
    wait_bytes(RX.at[pl.ds(0, NQ - 1)], wrs.at[0])

    def partial_sum(n, zd):
        cols = pl.ds(pl.multiple_of(n * FC, FC), FC)
        return jnp.dot(CM[zd], RX[:, :, cols].reshape(NQ * ROWS, FC), preferred_element_type=F32)

    def send_sum(n, s, d):
        odd = lax.rem(n, 2)
        ahead = (4 - odd if d == 0 else 3 + odd) - s
        zd = wrap(z + ahead, NZ) if d == 0 else wrap(z - ahead, NZ)
        value = partial_sum(n, zd)
        if s > 0:
            before = hop(s - 1, d)
            s_copy(n, before, d).wait_recv()
            value = value + RR[n, before].astype(F32)
        SR[n, hop(s, d)] = value.astype(BF16)
        s_copy(n, hop(s, d), d).start()

    for s in range(4):

        def send_step(n, _):
            for d in range(2):
                if s < 3:
                    send_sum(n, s, d)
                else:

                    @pl.when(lax.rem(n, 2) == d)
                    def _():
                        send_sum(n, s, d)

            return 0

        lax.fori_loop(0, NB, send_step, 0)

    def finish(n, _):
        odd = lax.rem(n, 2)
        value = partial_sum(n, z)
        for d in range(2):
            last = jnp.where(odd == d, 6, 4 + d)
            s_copy(n, last, d).wait_recv()
            value = value + RR[n, last].astype(F32)
        out_ref[:, pl.ds(pl.multiple_of(n * FC, FC), FC)] = value.astype(BF16)
        return 0

    lax.fori_loop(0, NB, finish, 0)

    wait_bytes(PM.at[pl.ds(1, NY - 1)], mrs.at[0])

    def mix(u, _):
        cols = pl.ds(pl.multiple_of(u * 512, 512), 512)
        value = PT[y, :, cols].astype(F32)
        for i in range(1, NY):
            value = value + PM[i, :, cols].astype(F32)
        mix_ref[:, cols] = value.astype(BF16)
        return 0

    lax.fori_loop(0, D // 512, mix, 0)

    for view, sem in (
        (G.at[:, pl.ds(0, 7)], zss),
        (IR.at[pl.ds(0, 7)], iss),
        (XS.at[:, pl.ds(0, NQ - 1)], xss),
        (XO, yss),
        (DN.at[pl.ds(0, NY - 1)], dss),
        (ACT.at[pl.ds(0, NY - 1)], ass),
        (RX.at[pl.ds(0, NQ - 1)], wss),
        (SR, sss),
        (PM.at[pl.ds(1, NY - 1)], mss),
        (KP, hss),
    ):
        wait_bytes(view, sem.at[0])


def write_out(mix_in, out_in, mix_ref, out_ref):
    mix_ref[...] = mix_in[...]
    out_ref[...] = out_in[...]


def shards(
    projected_queries,
    key_proj,
    projected_values,
    head_sink_logits,
    out_weight,
    expert_input,
    norm_gain,
    routing,
    route_weight,
    gate_weight,
    up_weight,
    down_weight,
):
    vmem = pl.BlockSpec(memory_space=pltpu.VMEM)
    hbm = pl.BlockSpec(memory_space=pl.ANY)
    smem = pl.BlockSpec(memory_space=pltpu.SMEM)
    dma = pltpu.SemaphoreType.DMA
    mixed, combined = pl.pallas_call(
        kernel,
        out_shape=(
            jax.ShapeDtypeStruct((64, D), BF16),
            jax.ShapeDtypeStruct((TOK, 1024), BF16),
        ),
        in_specs=[hbm, hbm, hbm, smem, hbm, hbm, hbm, hbm, hbm, hbm, hbm, hbm],
        out_specs=(vmem, vmem),
        scratch_shapes=[
            pltpu.VMEM((256, 512), BF16),
            pltpu.VMEM((256, 128), BF16),
            pltpu.VMEM((256, 128), BF16),
            pltpu.VMEM((TOK, D), BF16),
            pltpu.VMEM((1, D), F32),
            pltpu.VMEM((4, TOK), jnp.int32),
            pltpu.VMEM((4, TOK), F32),
            pltpu.VMEM((C, NZ, TOK, FC), BF16),
            pltpu.VMEM((C, NQ, ROWS, FC), BF16),
            pltpu.VMEM((C, NQ, ROWS, FC), BF16),
            pltpu.VMEM((CE, NQ, ROWS, FC), BF16),
            pltpu.VMEM((D // FC, FC, 2 * HID), BF16),
            pltpu.VMEM((512, D), BF16),
            pltpu.VMEM((NY, HID, 1024), BF16),
            pltpu.VMEM((NQ, ROWS, NZ * TOK), BF16),
            pltpu.VMEM((NZ, TOK, NQ * ROWS), BF16),
            pltpu.VMEM((NZ, 8, TOK), F32),
            pltpu.VMEM((NZ, 16, TOK), F32),
            pltpu.VMEM((NQ * ROWS, 2 * HID), F32),
            pltpu.VMEM((NY, NQ, ROWS, HID), BF16),
            pltpu.VMEM((NQ, ROWS, 1024), BF16),
            pltpu.VMEM((NQ, ROWS, 1024), BF16),
            pltpu.VMEM((NB, 7, TOK, FC), BF16),
            pltpu.VMEM((NB, 7, TOK, FC), BF16),
            pltpu.VMEM((2, 128, 128), BF16),
            pltpu.VMEM((2, 2, 384, 128), BF16),
            pltpu.VMEM((2, 2, 384, 128), BF16),
            pltpu.VMEM((256, 512), BF16),
            pltpu.VMEM((NY, 64, D), BF16),
            pltpu.VMEM((NY, 64, D), BF16),
            dma((11,)),
            dma((1,)), dma((C, 7)),
            dma((1,)), dma((7,)),
            dma((1,)), dma((C,)),
            dma((1,)), dma((CE,)),
            dma((1,)), dma((1,)),
            dma((1,)), dma((4,)),
            dma((1,)), dma((1,)),
            dma((1,)), dma((NB, 7)),
            dma((1,)), dma((1,)),
            dma((1,)), dma((1,)),
        ],
        compiler_params=pltpu.CompilerParams(
            collective_id=0, has_side_effects=True, vmem_limit_bytes=62 * 1024 * 1024
        ),
    )(
        projected_queries,
        key_proj,
        projected_values,
        head_sink_logits,
        out_weight,
        expert_input,
        norm_gain.reshape(1, D),
        routing.T,
        route_weight.T,
        gate_weight.reshape(D // FC, FC, HID),
        up_weight.reshape(D // FC, FC, HID),
        down_weight.reshape(HID, D),
    )
    return pl.pallas_call(
        write_out,
        out_shape=(
            jax.ShapeDtypeStruct((64, D), BF16),
            jax.ShapeDtypeStruct((TOK, 1024), BF16),
        ),
        in_specs=[vmem, vmem],
        out_specs=(vmem, vmem),
    )(mixed, combined)


def solution(mesh):
    placed = (
        P("ep", "tp"),
        P("ep", "tp"),
        P("ep", "tp"),
        P("tp"),
        P("tp", None),
        P("ep", None),
        P(),
        P("ep", None),
        P("ep", None),
        P("ep", None, "tp"),
        P("ep", None, "tp"),
        P("ep", "tp", None),
    )
    return jax.shard_map(
        shards,
        mesh=mesh,
        in_specs=placed,
        out_specs=(P(("ep", "tp"), None), P("ep", "tp")),
        check_vma=False,
    )
```

```python
import jax
import jax.numpy as jnp
from jax import lax
from jax.experimental import pallas as pl
from jax.experimental.pallas import tpu as pltpu
from jax.sharding import PartitionSpec as P

EPS = 1e-06
CLAMP = 7.0
SLOPE = 1.702

NZ = 8
NQ = 8
NY = 4
D = 4096
TOK = 128
CAP = 12
ROWS = NZ * CAP
FC = 256
CE = 7
C = 9
AHEAD = 3
HID = 256
NB = 4
HALF = ROWS // 2
PLACE = (7, 5, 3, 1, 0, 2, 4, 6)
OWN = 7
MESH = pl.DeviceIdType.MESH
F32 = jnp.float32
BF16 = jnp.bfloat16


def kernel(
    q_hbm, k_hbm, v_hbm, sink_ref, wo_hbm, x_hbm, gain_hbm, rt_hbm, rw_hbm, wg_hbm, wu_hbm, wd_hbm,
    mix_ref, out_ref,
    q_ref, k_ref, v_ref, x_ref, gain_ref, rt_ref, rw_ref,
    G, XS, XF, XO, W, WO, DN, S, CM, IR, RANK, ACC, ACT, YS, RX, SR, RR,
    KP, KX, VX, ATT, PT, PM, PN,
    ls, zss, zrs, iss, irs, xss, xrs, yss, yrs, dss, drs, ass, ars, wss, wrs, sss, srs, mss, mrs, hss, hrs,
):
    ep = lax.axis_index("ep")
    y = lax.axis_index("tp")
    z = ep // NQ
    q = lax.rem(ep, NQ)
    half = lax.rem(y, 2)

    def wrap(a, n):
        return lax.rem(a + n, n)

    def at_z(zz):
        return (zz * NQ + q, y)

    def at_q(qq):
        return (z * NQ + qq, y)

    def at_y(yy):
        return (ep, yy)

    def remote(src, dst, ss, rs, dev):
        return pltpu.make_async_remote_copy(src, dst, ss, rs, device_id=dev, device_id_type=MESH)

    barrier = pltpu.get_barrier_semaphore()
    next_ep, prev_ep = wrap(ep + 1, NZ * NQ), wrap(ep - 1, NZ * NQ)
    for i in (1, NZ - 1):
        pl.semaphore_signal(barrier, inc=1, device_id=at_z(wrap(z + i, NZ)), device_id_type=MESH)
    for i in range(1, NQ):
        pl.semaphore_signal(barrier, inc=1, device_id=at_q(wrap(q + i, NQ)), device_id_type=MESH)
    for i in range(1, NY):
        pl.semaphore_signal(barrier, inc=1, device_id=at_y(wrap(y + i, NY)), device_id_type=MESH)
    for e in (next_ep, prev_ep):
        pl.semaphore_signal(barrier, inc=1, device_id=(e, y), device_id_type=MESH)

    own_down = wd_hbm.at[:, pl.ds(pl.multiple_of(y * 1024, 1024), 1024)]
    pairs = (
        (x_hbm, x_ref), (gain_hbm, gain_ref), (rt_hbm, rt_ref), (rw_hbm, rw_ref),
        (k_hbm, k_ref), (v_hbm, v_ref), (q_hbm, q_ref),
        (wg_hbm, W.at[:, :, pl.ds(0, HID)]), (wu_hbm, W.at[:, :, pl.ds(HID, HID)]), (wo_hbm, WO), (own_down, DN.at[y]),
    )
    loads = [pltpu.make_async_copy(src, dst, ls.at[i]) for i, (src, dst) in enumerate(pairs)]
    for load in loads:
        load.start()

    def chunk(j):
        return jnp.where(j < CE, half * CE + j, CE + j)

    loads[0].wait()

    def mean_step(j, total):
        w = x_ref[:, pl.ds(pl.multiple_of(j * 512, 512), 512)].astype(F32)
        w = w * w
        return total + ((w[:, 0:128] + w[:, 128:256]) + (w[:, 256:384] + w[:, 384:512]))

    total = lax.fori_loop(0, D // 512, mean_step, jnp.zeros((TOK, 128), F32))
    scale = lax.rsqrt(jnp.sum(total, axis=1, keepdims=True) * (1.0 / D) + EPS)
    for i in (1, 2, 3):
        loads[i].wait()

    def norm_step(j, _):
        cols = pl.ds(pl.multiple_of(chunk(j) * FC, FC), FC)
        G[j, OWN] = (x_ref[:, cols].astype(F32) * scale * gain_ref[:, cols]).astype(BF16)
        return 0

    lax.fori_loop(0, C, norm_step, 0)
    IR[OWN] = jnp.concatenate([rt_ref[...].astype(F32), rw_ref[...]], axis=0)

    def hop(s, d):
        return 6 if s == 3 else 2 * s + d

    def ring(s, d):
        if d == 0:
            return PLACE[-s % NZ], PLACE[-(s + 1) % NZ], at_z(wrap(z + 1, NZ))
        return PLACE[s], PLACE[s + 1], at_z(wrap(z - 1, NZ))

    def z_copy(j, s, d):
        here, there, to = ring(s, d)
        return remote(G.at[j, here], G.at[j, there], zss.at[0], zrs.at[j, hop(s, d)], to)

    def i_copy(s, d):
        here, there, to = ring(s, d)
        return remote(IR.at[here], IR.at[there], iss.at[0], irs.at[hop(s, d)], to)

    def x_copy(j, to):
        return remote(XS.at[j, to], XF.at[j, q], xss.at[0], xrs.at[j], at_q(to))

    def y_copy(j, d):
        to = wrap(y + 1, NY) if d == 0 else wrap(y - 1, NY)
        part = pl.ds(4 * d, 4)
        return remote(XF.at[j, part], XO.at[j, part], yss.at[0], yrs.at[j], at_y(to))

    def d_copy(i):
        to = wrap(y + i, NY)
        src = wd_hbm.at[:, pl.ds(pl.multiple_of(to * 1024, 1024), 1024)]
        return remote(src, DN.at[y], dss.at[0], drs.at[0], at_y(to))

    def a_copy(h, qq, b, i):
        to = wrap(y + i, NY)
        return remote(ACT.at[y, h, qq], ACT.at[y, h, qq], ass.at[0], ars.at[4 * h + b], at_y(to))

    def w_copy(h, to):
        return remote(YS.at[h, to], RX.at[h, q], wss.at[0], wrs.at[h], at_q(to))

    def s_copy(n, h, d):
        peer = wrap(z + 1, NZ) if d == 0 else wrap(z - 1, NZ)
        return remote(SR.at[n, h], RR.at[n, h], sss.at[0], srs.at[n, h], at_z(peer))

    def m_copy(step, d):
        to = wrap(y + 1, NY) if d == 0 else wrap(y - 1, NY)
        if step == 0:
            return remote(PT.at[wrap(y + 2, NY), d], PM.at[d], mss.at[0], mrs.at[d], at_y(to))
        return remote(PT.at[to], PN.at[d], mss.at[1], mrs.at[2 + d], at_y(to))

    halo = [
        remote(k_hbm.at[pl.ds(128, 128)], KP.at[0], hss.at[0], hrs.at[0], (next_ep, y)),
        remote(v_hbm.at[pl.ds(128, 128)], KP.at[1], hss.at[0], hrs.at[0], (next_ep, y)),
    ]

    def wait_bytes(view, sem):
        pltpu.make_async_copy(view, view, sem).wait()

    pl.semaphore_wait(barrier, 2 + (NQ - 1) + (NY - 1) + 2)
    for d in range(2):
        z_copy(0, 0, d).start()
        i_copy(0, d).start()
    for j in range(1, AHEAD):
        for d in range(2):
            z_copy(j, 0, d).start()
    for copy in halo:
        copy.start()
    for i in (2, 1, 3):
        d_copy(i).start()
    ACC[...] = jnp.zeros_like(ACC)

    def widen(whole, wide, rows):
        lanes = lax.broadcasted_iota(jnp.int32, whole.shape, 1)
        whole = whole.astype(F32)
        turned = pltpu.roll(whole, 64, 1)
        zero = jnp.zeros_like(whole)
        wide[0, 0, rows, :] = jnp.where(lanes < 64, whole, zero).astype(BF16)
        wide[1, 1, rows, :] = jnp.where(lanes < 64, zero, whole).astype(BF16)
        wide[0, 1, rows, :] = jnp.where(lanes < 64, zero, turned).astype(BF16)
        wide[1, 0, rows, :] = jnp.where(lanes < 64, turned, zero).astype(BF16)

    def own_windows():
        for i in (4, 5, 6):
            loads[i].wait()
        widen(k_ref[...], KX, pl.ds(128, 256))
        widen(v_ref[...], VX, pl.ds(128, 256))

    def prior_windows():
        wait_bytes(KP, hrs.at[0])
        widen(KP[0], KX, pl.ds(0, 128))
        widen(KP[1], VX, pl.ds(0, 128))

    def div12(a):
        return (a * 5462) >> 16

    def build_gather():
        u = lax.broadcasted_iota(jnp.int32, (TOK, TOK), 0)
        t = lax.broadcasted_iota(jnp.int32, (TOK, TOK), 1)
        earlier = (u < t).astype(F32).astype(BF16)
        expert = (lax.broadcasted_iota(jnp.int32, (NQ, TOK), 0) + z * NQ).astype(F32)
        named, weight = [], []
        for zs in range(NZ):
            info = IR[zs]
            hits = [(info[k : k + 1, :] == expert).astype(F32) for k in range(4)]
            named.append(hits[0] + hits[1] + hits[2] + hits[3])
            weight.append(sum(hits[k] * info[4 + k : 5 + k, :] for k in range(4)))
        named = jnp.concatenate(named, axis=0)
        rank = jnp.dot(named.astype(BF16), earlier, preferred_element_type=F32)
        rank = jnp.where(named > 0.5, rank, -1.0)
        for zs in range(NZ):
            RANK[zs, 0:8, :] = rank[8 * zs : 8 * zs + 8, :]
            RANK[zs, 8:16, :] = weight[zs]
        row = lax.broadcasted_iota(jnp.int32, (ROWS, 128), 0)
        row_p = div12(row)
        row_k = (row - row_p * CAP).astype(F32)

        def step(zs, _):
            cols = pl.ds(pl.multiple_of(zs * TOK, TOK), TOK)
            ranks = RANK[zs, 0:8, :]
            for e in range(NQ):
                hit = (row_p == zs) & (ranks[e : e + 1, :] == row_k)
                S[e, :, cols] = hit.astype(F32).astype(BF16)
            return 0

        lax.fori_loop(0, NZ, step, 0)

    def build_combine():
        i16 = lax.broadcasted_iota(jnp.int32, (16, NQ * HALF), 0)
        col_q = div12(lax.broadcasted_iota(jnp.int32, (16, NQ * HALF), 1)) >> 2
        spread_rank = (i16 == col_q).astype(F32).astype(BF16)
        spread_weight = (i16 == col_q + 8).astype(F32).astype(BF16)
        col = lax.broadcasted_iota(jnp.int32, (TOK, NQ * HALF), 1)
        col12 = div12(col)
        col_p = col12 & 3
        col_k = (col - col12 * CAP).astype(F32)

        def step(p, _):
            turned = RANK[p].T.astype(BF16)
            ranks = jnp.dot(turned, spread_rank, preferred_element_type=F32)
            weights = jnp.dot(turned, spread_weight, preferred_element_type=F32)
            hit = (col_p == (p & 3)) & (ranks == col_k)
            CM[p] = jnp.where(hit, weights, 0.0).astype(BF16)
            return 0

        lax.fori_loop(0, NZ, step, 0)

    def attend(u):
        n, p = u // 4, lax.rem(u, 4)
        kv = p // 2
        rows = pl.ds(pl.multiple_of(n * 128, 128), 128)
        window = pl.ds(pl.multiple_of(n * 128, 128), 256)
        cols = pl.ds(pl.multiple_of(p * 128, 128), 128)
        queries = q_ref[rows, cols]
        i = lax.broadcasted_iota(jnp.int32, (128, 256), 0)
        s = lax.broadcasted_iota(jnp.int32, (128, 256), 1)
        first = jnp.where((ep == 0) & (n == 0), 128, 0)
        seen = (s > i) & (s <= i + 128) & (s >= first)
        both = jnp.zeros((128, 128), F32)
        for h in range(2):
            scores = lax.dot_general(
                queries, KX[kv, h, window, :], (((1,), (1,)), ((), ())), preferred_element_type=F32
            ) * 0.125
            scores = jnp.where(seen, scores, -jnp.inf)
            sink = sink_ref[2 * p + h]
            highest = jnp.maximum(jnp.max(scores, axis=1, keepdims=True), sink)
            e = jnp.exp(scores - highest)
            under = jnp.sum(e, axis=1, keepdims=True) + jnp.exp(sink - highest)
            w = (e / under).astype(BF16)
            both = both + jnp.dot(w, VX[kv, h, window, :], preferred_element_type=F32)
        ATT[rows, cols] = both.astype(BF16)

    def project(u):
        cols = pl.ds(pl.multiple_of(u * 512, 512), 512)
        part = jnp.dot(ATT[...], WO[:, cols], preferred_element_type=F32).astype(BF16)
        inner = pl.ds(pl.multiple_of(lax.rem(u, 4) * 512, 512), 512)
        PT[:, u // 4, :, inner] = part.reshape(NY, 64, 512)

    def expert_dots(*terms):
        def step(r, _):
            part = pl.ds(4 * r, 4)
            rows = pl.ds(pl.multiple_of(r * 4 * ROWS, 4 * ROWS), 4 * ROWS)
            value = ACC[rows, :]
            for src, j, w in terms:
                block = src[j, part].reshape(4 * ROWS, FC)
                value = value + jnp.dot(block, W[w], preferred_element_type=F32)
            ACC[rows, :] = value
            return 0

        lax.fori_loop(0, 2, step, 0)

    def within(j):
        return (j >= 0) & (j < C)

    def pick(j, r):
        part = pl.ds(4 * r, 4)
        block = jnp.dot(
            S[part].reshape(4 * ROWS, NZ * TOK), G[j].reshape(NZ * TOK, FC), preferred_element_type=F32
        ).astype(BF16)
        XS[j, part] = block.reshape(4, ROWS, FC)
        for i in range(4):

            @pl.when(4 * r + i != q)
            def _():
                x_copy(j, 4 * r + i).start()

    def tick(t, _):
        @pl.when(within(t - 3))
        def _():
            j = t - 3

            @pl.when(j == 0)
            def _():
                i_copy(2, 0).wait_recv()
                i_copy(2, 1).wait_recv()
                i_copy(3, 0).start()

            for d in range(2):
                z_copy(j, 2, d).wait_recv()

                @pl.when(lax.rem(j, 2) == d)
                def _():
                    z_copy(j, 3, d).start()

        @pl.when(within(t - 4))
        def _():
            j = t - 4

            @pl.when(j == 0)
            def _():
                i_copy(3, 0).wait_recv()
                build_gather()

            for d in range(2):

                @pl.when(lax.rem(j, 2) == d)
                def _():
                    z_copy(j, 3, d).wait_recv()

            pick(j, 0)

        for s in (2, 1):

            @pl.when(within(t - s))
            def _():
                for d in range(2):

                    @pl.when(t == s)
                    def _():
                        i_copy(s - 1, d).wait_recv()
                        i_copy(s, d).start()

                    z_copy(t - s, s - 1, d).wait_recv()
                    z_copy(t - s, s, d).start()

            if s == 2:

                @pl.when(within(t - 4))
                def _():
                    pick(t - 4, 1)
                    XF[t - 4, q] = XS[t - 4, q]

        @pl.when(t == 1)
        def _():
            for d in range(2):
                z_copy(AHEAD, 0, d).start()

        @pl.when((t > 0) & (t + AHEAD < C))
        def _():
            for d in range(2):
                z_copy(t + AHEAD, 0, d).start()

        @pl.when(within(t - 6))
        def _():
            j = t - 6
            wait_bytes(XF.at[j, pl.ds(0, NQ - 1)], xrs.at[j])

            @pl.when(j < CE)
            def _():
                for d in range(2):
                    y_copy(j, d).start()

            @pl.when(j == 0)
            def _():
                loads[7].wait()
                loads[8].wait()

        @pl.when((t >= 6) & (t < 8))
        def _():
            expert_dots((XF, t - 6, chunk(t - 6)))

        @pl.when((t >= 8) & (t < 8 + CE))
        def _():
            j = t - 8
            wait_bytes(XO.at[j], yrs.at[j])
            expert_dots((XF, t - 6, chunk(t - 6)), (XO, j, (1 - half) * CE + j))

        @pl.when(t == 0)
        def _():
            own_windows()

        @pl.when(t == 2)
        def _():
            prior_windows()

        @pl.when((t == 1) | (t == 2))
        def _():
            for i in range(4):
                attend((2 - t) * 4 + i)

        @pl.when(t == 3)
        def _():
            loads[9].wait()

        @pl.when((t == 3) | (t == 4))
        def _():
            for i in range(4):
                project((t - 3) * 4 + i)

        @pl.when(t == 4)
        def _():
            for d in range(2):
                m_copy(0, d).start()

        return 0

    lax.fori_loop(0, C + 6, tick, 0)

    def pair(b):
        chip, core = q // 2, lax.rem(q, 2)
        apart = (b > 0) & (b < 3)
        dx = jnp.where(b == 0, 2, jnp.where(b == 3, 0, 1))
        dc = jnp.where(apart, b - 1, 0)
        first = lax.rem(chip + dx, 4) * 2 + lax.rem(core + dc, 2)
        dx = jnp.where(apart, 3, dx)
        dc = jnp.where(apart, b - 1, 1)
        return first, lax.rem(chip + dx, 4) * 2 + lax.rem(core + dc, 2)

    def activate(hb, _):
        h, b = hb // 4, lax.rem(hb, 4)
        for qq in pair(b):
            rows = pl.ds(pl.multiple_of(qq * ROWS + h * HALF, 16), HALF)
            g = jnp.minimum(ACC[rows, 0:HID], CLAMP)
            u = jnp.clip(ACC[rows, HID : 2 * HID], -CLAMP, CLAMP) + 1.0
            ACT[y, h, qq] = (u * g * jax.nn.sigmoid(SLOPE * g)).astype(BF16)
            for i in (2, 1, 3):
                a_copy(h, qq, b, i).start()
        return 0

    lax.fori_loop(0, 8, activate, 0)
    build_combine()
    loads[10].wait()
    wait_bytes(DN.at[pl.ds(0, NY - 1)], drs.at[0])
    for d in range(2):
        wait_bytes(PM.at[d], mrs.at[d])
        to = wrap(y + 1, NY) if d == 0 else wrap(y - 1, NY)
        PT[to, d] = (PT[to, d].astype(F32) + PM[d].astype(F32)).astype(BF16)

    def down(hb, _):
        h, b = hb // 4, lax.rem(hb, 4)
        wait_bytes(ACT.at[pl.ds(0, NY - 1), 0, pl.ds(0, 2)], ars.at[hb])
        qs = pair(b)
        block = jnp.zeros((2 * HALF, 1024), F32)
        for i in range(NY):
            acts = jnp.concatenate([ACT[i, h, qq] for qq in qs], axis=0)
            block = block + jnp.dot(acts, DN[i], preferred_element_type=F32)
        for i, qq in enumerate(qs):
            YS[h, qq] = block[i * HALF : (i + 1) * HALF].astype(BF16)

            @pl.when(qq != q)
            def _():
                w_copy(h, qq).start()

            @pl.when(qq == q)
            def _():
                RX[h, q] = YS[h, q]

        return 0

    lax.fori_loop(0, 6, down, 0)
    wait_bytes(RX.at[0, pl.ds(0, NQ - 1)], wrs.at[0])

    def partial_sum(n, place):
        cols = pl.ds(pl.multiple_of(n * FC, FC), FC)
        rows = RX[place // 4, :, :, cols].reshape(NQ * HALF, FC)
        return jnp.dot(CM[place], rows, preferred_element_type=F32)

    def send_sum(n, s, d):
        odd = lax.rem(n, 2)
        if d == 0:
            ahead = 4 - odd - s
            place = jnp.where(ahead == 4, 0, 2 * (4 - ahead) - 1)
        else:
            ahead = 3 + odd - s
            place = 2 * (4 - ahead)
        value = partial_sum(n, place)
        if s > 0:
            before = hop(s - 1, d)
            s_copy(n, before, d).wait_recv()
            value = value + RR[n, before].astype(F32)
        SR[n, hop(s, d)] = value.astype(BF16)
        s_copy(n, hop(s, d), d).start()

    def over_chunks(body):
        def step(n, _):
            body(n)
            return 0

        lax.fori_loop(0, NB, step, 0)

    def first(n):
        send_sum(n, 0, 0)
        send_sum(n, 0, 1)

    def most(s):
        def body(n):
            send_sum(n, s, 0)

            @pl.when(lax.rem(n, 2) == 1)
            def _():
                send_sum(n, s, 1)

        return body

    def rest(s):
        def body(n):
            @pl.when(lax.rem(n, 2) == 0)
            def _():
                send_sum(n, s, 1)

        return body

    def fourth(n):
        for d in range(2):

            @pl.when(lax.rem(n, 2) == d)
            def _():
                send_sum(n, 3, d)

    def finish(n):
        value = partial_sum(n, OWN)
        for d in range(2):
            last = jnp.where(lax.rem(n, 2) == d, 6, 4 + d)
            s_copy(n, last, d).wait_recv()
            value = value + RR[n, last].astype(F32)
        out_ref[:, pl.ds(pl.multiple_of(n * FC, FC), FC)] = value.astype(BF16)

    over_chunks(first)
    lax.fori_loop(6, 8, down, 0)
    for d in range(2):
        m_copy(1, d).start()
    over_chunks(most(1))
    wait_bytes(RX.at[1, pl.ds(0, NQ - 1)], wrs.at[1])
    over_chunks(rest(1))
    over_chunks(most(2))
    over_chunks(rest(2))
    over_chunks(fourth)

    wait_bytes(PN.at[0], mrs.at[2])
    wait_bytes(PN.at[1], mrs.at[3])

    def mix(u, _):
        c, cols = u // 4, pl.ds(pl.multiple_of(lax.rem(u, 4) * 512, 512), 512)
        value = PT[y, c, :, cols].astype(F32) + PN[0, c, :, cols].astype(F32) + PN[1, c, :, cols].astype(F32)
        mix_ref[:, pl.ds(pl.multiple_of(u * 512, 512), 512)] = value.astype(BF16)
        return 0

    lax.fori_loop(0, D // 512, mix, 0)
    over_chunks(finish)

    for view, sem in (
        (G.at[:, pl.ds(0, 7)], zss),
        (IR.at[pl.ds(0, 7)], iss),
        (XS.at[:, pl.ds(0, NQ - 1)], xss),
        (XO, yss),
        (DN.at[pl.ds(0, NY - 1)], dss),
        (ACT.at[pl.ds(0, NY - 1)], ass),
        (RX.at[:, pl.ds(0, NQ - 1)], wss),
        (SR, sss),
        (PM, mss),
        (KP, hss),
    ):
        wait_bytes(view, sem.at[0])
    wait_bytes(PN, mss.at[1])


def write_out(mix_in, out_in, mix_ref, out_ref):
    mix_ref[...] = mix_in[...]
    out_ref[...] = out_in[...]


def shards(
    projected_queries,
    key_proj,
    projected_values,
    head_sink_logits,
    out_weight,
    expert_input,
    norm_gain,
    routing,
    route_weight,
    gate_weight,
    up_weight,
    down_weight,
):
    vmem = pl.BlockSpec(memory_space=pltpu.VMEM)
    hbm = pl.BlockSpec(memory_space=pl.ANY)
    smem = pl.BlockSpec(memory_space=pltpu.SMEM)
    dma = pltpu.SemaphoreType.DMA
    mixed, combined = pl.pallas_call(
        kernel,
        out_shape=(
            jax.ShapeDtypeStruct((64, D), BF16),
            jax.ShapeDtypeStruct((TOK, 1024), BF16),
        ),
        in_specs=[hbm, hbm, hbm, smem, hbm, hbm, hbm, hbm, hbm, hbm, hbm, hbm],
        out_specs=(vmem, vmem),
        scratch_shapes=[
            pltpu.VMEM((256, 512), BF16),
            pltpu.VMEM((256, 128), BF16),
            pltpu.VMEM((256, 128), BF16),
            pltpu.VMEM((TOK, D), BF16),
            pltpu.VMEM((1, D), F32),
            pltpu.VMEM((4, TOK), jnp.int32),
            pltpu.VMEM((4, TOK), F32),
            pltpu.VMEM((C, NZ, TOK, FC), BF16),
            pltpu.VMEM((C, NQ, ROWS, FC), BF16),
            pltpu.VMEM((C, NQ, ROWS, FC), BF16),
            pltpu.VMEM((CE, NQ, ROWS, FC), BF16),
            pltpu.VMEM((D // FC, FC, 2 * HID), BF16),
            pltpu.VMEM((512, D), BF16),
            pltpu.VMEM((NY, HID, 1024), BF16),
            pltpu.VMEM((NQ, ROWS, NZ * TOK), BF16),
            pltpu.VMEM((NZ, TOK, NQ * HALF), BF16),
            pltpu.VMEM((NZ, 8, TOK), F32),
            pltpu.VMEM((NZ, 16, TOK), F32),
            pltpu.VMEM((NQ * ROWS, 2 * HID), F32),
            pltpu.VMEM((NY, 2, NQ, HALF, HID), BF16),
            pltpu.VMEM((2, NQ, HALF, 1024), BF16),
            pltpu.VMEM((2, NQ, HALF, 1024), BF16),
            pltpu.VMEM((NB, 7, TOK, FC), BF16),
            pltpu.VMEM((NB, 7, TOK, FC), BF16),
            pltpu.VMEM((2, 128, 128), BF16),
            pltpu.VMEM((2, 2, 384, 128), BF16),
            pltpu.VMEM((2, 2, 384, 128), BF16),
            pltpu.VMEM((256, 512), BF16),
            pltpu.VMEM((NY, 2, 64, D // 2), BF16),
            pltpu.VMEM((2, 64, D // 2), BF16),
            pltpu.VMEM((2, 2, 64, D // 2), BF16),
            dma((11,)),
            dma((1,)), dma((C, 7)),
            dma((1,)), dma((7,)),
            dma((1,)), dma((C,)),
            dma((1,)), dma((CE,)),
            dma((1,)), dma((1,)),
            dma((1,)), dma((8,)),
            dma((1,)), dma((2,)),
            dma((1,)), dma((NB, 7)),
            dma((2,)), dma((4,)),
            dma((1,)), dma((1,)),
        ],
        compiler_params=pltpu.CompilerParams(
            collective_id=0, has_side_effects=True, vmem_limit_bytes=62 * 1024 * 1024
        ),
    )(
        projected_queries,
        key_proj,
        projected_values,
        head_sink_logits,
        out_weight,
        expert_input,
        norm_gain.reshape(1, D),
        routing.T,
        route_weight.T,
        gate_weight.reshape(D // FC, FC, HID),
        up_weight.reshape(D // FC, FC, HID),
        down_weight.reshape(HID, D),
    )
    return pl.pallas_call(
        write_out,
        out_shape=(
            jax.ShapeDtypeStruct((64, D), BF16),
            jax.ShapeDtypeStruct((TOK, 1024), BF16),
        ),
        in_specs=[vmem, vmem],
        out_specs=(vmem, vmem),
    )(mixed, combined)


def solution(mesh):
    placed = (
        P("ep", "tp"),
        P("ep", "tp"),
        P("ep", "tp"),
        P("tp"),
        P("tp", None),
        P("ep", None),
        P(),
        P("ep", None),
        P("ep", None),
        P("ep", None, "tp"),
        P("ep", None, "tp"),
        P("ep", "tp", None),
    )
    return jax.shard_map(
        shards,
        mesh=mesh,
        in_specs=placed,
        out_specs=(P(("ep", "tp"), None), P("ep", "tp")),
        check_vma=False,
    )
```

```python
import jax
import jax.numpy as jnp
from jax import lax
from jax.experimental import pallas as pl
from jax.experimental.pallas import tpu as pltpu
from jax.sharding import PartitionSpec as P

EPS = 1e-06
CLAMP = 7.0
SLOPE = 1.702

NZ = 8
NQ = 8
NY = 4
D = 4096
TOK = 128
CAP = 12
ROWS = NZ * CAP
FC = 256
CE = 7
C = 9
AHEAD = 3
HID = 256
NB = 4
HALF = ROWS // 2
PLACE = (7, 5, 3, 1, 0, 2, 4, 6)
OWN = 7
MESH = pl.DeviceIdType.MESH
F32 = jnp.float32
BF16 = jnp.bfloat16


def kernel(
    q_hbm, k_hbm, v_hbm, sink_ref, wo_hbm, x_hbm, gain_hbm, rt_hbm, rw_hbm, wg_hbm, wu_hbm, wd_hbm,
    mix_ref, out_ref,
    q_ref, k_ref, v_ref, x_ref, gain_ref, rt_ref, rw_ref,
    G, XS, XF, XO, W, WO, DN, S, CM, IR, RANK, ACC, ACT, YS, RX, SR, RR,
    KP, KX, VX, ATT, PT, PM, PN,
    ls, zss, zrs, iss, irs, xss, xrs, yss, yrs, dss, drs, ass, ars, wss, wrs, sss, srs, mss, mrs, hss, hrs,
):
    ep = lax.axis_index("ep")
    y = lax.axis_index("tp")
    z = ep // NQ
    q = lax.rem(ep, NQ)
    half = lax.rem(y, 2)

    def wrap(a, n):
        return lax.rem(a + n, n)

    def at_z(zz):
        return (zz * NQ + q, y)

    def at_q(qq):
        return (z * NQ + qq, y)

    def at_y(yy):
        return (ep, yy)

    def remote(src, dst, ss, rs, dev):
        return pltpu.make_async_remote_copy(src, dst, ss, rs, device_id=dev, device_id_type=MESH)

    barrier = pltpu.get_barrier_semaphore()
    next_ep, prev_ep = wrap(ep + 1, NZ * NQ), wrap(ep - 1, NZ * NQ)
    for i in (1, NZ - 1):
        pl.semaphore_signal(barrier, inc=1, device_id=at_z(wrap(z + i, NZ)), device_id_type=MESH)
    for i in range(1, NQ):
        pl.semaphore_signal(barrier, inc=1, device_id=at_q(wrap(q + i, NQ)), device_id_type=MESH)
    for i in range(1, NY):
        pl.semaphore_signal(barrier, inc=1, device_id=at_y(wrap(y + i, NY)), device_id_type=MESH)
    for e in (next_ep, prev_ep):
        pl.semaphore_signal(barrier, inc=1, device_id=(e, y), device_id_type=MESH)

    own_down = wd_hbm.at[:, pl.ds(pl.multiple_of(y * 1024, 1024), 1024)]
    pairs = (
        (x_hbm, x_ref), (gain_hbm, gain_ref), (rt_hbm, rt_ref), (rw_hbm, rw_ref),
        (k_hbm, k_ref), (v_hbm, v_ref), (q_hbm, q_ref),
        (wg_hbm, W.at[:, :, pl.ds(0, HID)]), (wu_hbm, W.at[:, :, pl.ds(HID, HID)]), (wo_hbm, WO), (own_down, DN.at[y]),
    )
    loads = [pltpu.make_async_copy(src, dst, ls.at[i]) for i, (src, dst) in enumerate(pairs)]
    for load in loads:
        load.start()

    def chunk(j):
        return jnp.where(j < CE, half * CE + j, CE + j)

    loads[0].wait()

    def mean_step(j, total):
        w = x_ref[:, pl.ds(pl.multiple_of(j * 512, 512), 512)].astype(F32)
        w = w * w
        return total + ((w[:, 0:128] + w[:, 128:256]) + (w[:, 256:384] + w[:, 384:512]))

    total = lax.fori_loop(0, D // 512, mean_step, jnp.zeros((TOK, 128), F32))
    scale = lax.rsqrt(jnp.sum(total, axis=1, keepdims=True) * (1.0 / D) + EPS)
    for i in (1, 2, 3):
        loads[i].wait()

    def norm_step(j, _):
        cols = pl.ds(pl.multiple_of(chunk(j) * FC, FC), FC)
        G[j, OWN] = (x_ref[:, cols].astype(F32) * scale * gain_ref[:, cols]).astype(BF16)
        return 0

    lax.fori_loop(0, C, norm_step, 0)
    IR[OWN] = jnp.concatenate([rt_ref[...].astype(F32), rw_ref[...]], axis=0)

    def hop(s, d):
        return 6 if s == 3 else 2 * s + d

    def ring(s, d):
        if d == 0:
            return PLACE[-s % NZ], PLACE[-(s + 1) % NZ], at_z(wrap(z + 1, NZ))
        return PLACE[s], PLACE[s + 1], at_z(wrap(z - 1, NZ))

    def z_copy(j, s, d):
        here, there, to = ring(s, d)
        return remote(G.at[j, here], G.at[j, there], zss.at[0], zrs.at[j, hop(s, d)], to)

    def i_copy(s, d):
        here, there, to = ring(s, d)
        return remote(IR.at[here], IR.at[there], iss.at[0], irs.at[hop(s, d)], to)

    def x_copy(j, to):
        return remote(XS.at[j, to], XF.at[j, q], xss.at[0], xrs.at[j], at_q(to))

    def y_copy(j, d):
        to = wrap(y + 1, NY) if d == 0 else wrap(y - 1, NY)
        part = pl.ds(4 * d, 4)
        return remote(XF.at[j, part], XO.at[j, part], yss.at[0], yrs.at[j], at_y(to))

    def d_copy(i):
        to = wrap(y + i, NY)
        src = wd_hbm.at[:, pl.ds(pl.multiple_of(to * 1024, 1024), 1024)]
        return remote(src, DN.at[y], dss.at[0], drs.at[0], at_y(to))

    def a_copy(h, qq, b, i):
        to = wrap(y + i, NY)
        return remote(ACT.at[y, h, qq], ACT.at[y, h, qq], ass.at[0], ars.at[4 * h + b], at_y(to))

    def w_copy(h, to):
        return remote(YS.at[h, to], RX.at[h, q], wss.at[0], wrs.at[h], at_q(to))

    def s_copy(n, h, d):
        peer = wrap(z + 1, NZ) if d == 0 else wrap(z - 1, NZ)
        return remote(SR.at[n, h], RR.at[n, h], sss.at[0], srs.at[n, h], at_z(peer))

    def m_copy(step, d):
        to = wrap(y + 1, NY) if d == 0 else wrap(y - 1, NY)
        if step == 0:
            return remote(PT.at[wrap(y + 2, NY), d], PM.at[d], mss.at[0], mrs.at[d], at_y(to))
        return remote(PT.at[to], PN.at[d], mss.at[1], mrs.at[2 + d], at_y(to))

    halo = [
        remote(k_hbm.at[pl.ds(128, 128)], KP.at[0], hss.at[0], hrs.at[0], (next_ep, y)),
        remote(v_hbm.at[pl.ds(128, 128)], KP.at[1], hss.at[0], hrs.at[0], (next_ep, y)),
    ]

    def wait_bytes(view, sem):
        pltpu.make_async_copy(view, view, sem).wait()

    pl.semaphore_wait(barrier, 2 + (NQ - 1) + (NY - 1) + 2)
    for d in range(2):
        z_copy(0, 0, d).start()
        i_copy(0, d).start()
    for j in range(1, AHEAD):
        for d in range(2):
            z_copy(j, 0, d).start()
    for copy in halo:
        copy.start()
    for i in (2, 1, 3):
        d_copy(i).start()
    ACC[...] = jnp.zeros_like(ACC)

    def widen(whole, wide, rows):
        lanes = lax.broadcasted_iota(jnp.int32, whole.shape, 1)
        whole = whole.astype(F32)
        turned = pltpu.roll(whole, 64, 1)
        zero = jnp.zeros_like(whole)
        wide[0, 0, rows, :] = jnp.where(lanes < 64, whole, zero).astype(BF16)
        wide[1, 1, rows, :] = jnp.where(lanes < 64, zero, whole).astype(BF16)
        wide[0, 1, rows, :] = jnp.where(lanes < 64, zero, turned).astype(BF16)
        wide[1, 0, rows, :] = jnp.where(lanes < 64, turned, zero).astype(BF16)

    def own_windows():
        for i in (4, 5, 6):
            loads[i].wait()
        widen(k_ref[...], KX, pl.ds(128, 256))
        widen(v_ref[...], VX, pl.ds(128, 256))

    def prior_windows():
        wait_bytes(KP, hrs.at[0])
        widen(KP[0], KX, pl.ds(0, 128))
        widen(KP[1], VX, pl.ds(0, 128))

    def div12(a):
        return (a * 5462) >> 16

    def build_gather():
        u = lax.broadcasted_iota(jnp.int32, (TOK, TOK), 0)
        t = lax.broadcasted_iota(jnp.int32, (TOK, TOK), 1)
        earlier = (u < t).astype(F32).astype(BF16)
        expert = (lax.broadcasted_iota(jnp.int32, (NQ, TOK), 0) + z * NQ).astype(F32)
        named, weight = [], []
        for zs in range(NZ):
            info = IR[zs]
            hits = [(info[k : k + 1, :] == expert).astype(F32) for k in range(4)]
            named.append(hits[0] + hits[1] + hits[2] + hits[3])
            weight.append(sum(hits[k] * info[4 + k : 5 + k, :] for k in range(4)))
        named = jnp.concatenate(named, axis=0)
        rank = jnp.dot(named.astype(BF16), earlier, preferred_element_type=F32)
        rank = jnp.where(named > 0.5, rank, -1.0)
        for zs in range(NZ):
            RANK[zs, 0:8, :] = rank[8 * zs : 8 * zs + 8, :]
            RANK[zs, 8:16, :] = weight[zs]
        row = lax.broadcasted_iota(jnp.int32, (ROWS, 128), 0)
        row_p = div12(row)
        row_k = (row - row_p * CAP).astype(F32)

        def step(zs, _):
            cols = pl.ds(pl.multiple_of(zs * TOK, TOK), TOK)
            ranks = RANK[zs, 0:8, :]
            for e in range(NQ):
                hit = (row_p == zs) & (ranks[e : e + 1, :] == row_k)
                S[e, :, cols] = hit.astype(F32).astype(BF16)
            return 0

        lax.fori_loop(0, NZ, step, 0)

    def build_combine():
        i16 = lax.broadcasted_iota(jnp.int32, (16, NQ * HALF), 0)
        col_q = div12(lax.broadcasted_iota(jnp.int32, (16, NQ * HALF), 1)) >> 2
        spread_rank = (i16 == col_q).astype(F32).astype(BF16)
        spread_weight = (i16 == col_q + 8).astype(F32).astype(BF16)
        col = lax.broadcasted_iota(jnp.int32, (TOK, NQ * HALF), 1)
        col12 = div12(col)
        col_p = col12 & 3
        col_k = (col - col12 * CAP).astype(F32)

        def step(p, _):
            turned = RANK[p].T.astype(BF16)
            ranks = jnp.dot(turned, spread_rank, preferred_element_type=F32)
            weights = jnp.dot(turned, spread_weight, preferred_element_type=F32)
            hit = (col_p == (p & 3)) & (ranks == col_k)
            CM[p] = jnp.where(hit, weights, 0.0).astype(BF16)
            return 0

        lax.fori_loop(0, NZ, step, 0)

    def attend(u):
        n, p = u // 4, lax.rem(u, 4)
        kv = p // 2
        rows = pl.ds(pl.multiple_of(n * 128, 128), 128)
        window = pl.ds(pl.multiple_of(n * 128, 128), 256)
        cols = pl.ds(pl.multiple_of(p * 128, 128), 128)
        queries = q_ref[rows, cols]
        i = lax.broadcasted_iota(jnp.int32, (128, 256), 0)
        s = lax.broadcasted_iota(jnp.int32, (128, 256), 1)
        first = jnp.where((ep == 0) & (n == 0), 128, 0)
        seen = (s > i) & (s <= i + 128) & (s >= first)
        both = jnp.zeros((128, 128), F32)
        for h in range(2):
            scores = lax.dot_general(
                queries, KX[kv, h, window, :], (((1,), (1,)), ((), ())), preferred_element_type=F32
            ) * 0.125
            scores = jnp.where(seen, scores, -jnp.inf)
            sink = sink_ref[2 * p + h]
            highest = jnp.maximum(jnp.max(scores, axis=1, keepdims=True), sink)
            e = jnp.exp(scores - highest)
            under = jnp.sum(e, axis=1, keepdims=True) + jnp.exp(sink - highest)
            w = (e / under).astype(BF16)
            both = both + jnp.dot(w, VX[kv, h, window, :], preferred_element_type=F32)
        ATT[rows, cols] = both.astype(BF16)

    def project(u):
        cols = pl.ds(pl.multiple_of(u * 512, 512), 512)
        part = jnp.dot(ATT[...], WO[:, cols], preferred_element_type=F32).astype(BF16)
        inner = pl.ds(pl.multiple_of(lax.rem(u, 4) * 512, 512), 512)
        PT[:, u // 4, :, inner] = part.reshape(NY, 64, 512)

    def expert_dots(*terms):
        def step(r, _):
            part = pl.ds(4 * r, 4)
            rows = pl.ds(pl.multiple_of(r * 4 * ROWS, 4 * ROWS), 4 * ROWS)
            value = ACC[rows, :]
            for src, j, w in terms:
                block = src[j, part].reshape(4 * ROWS, FC)
                value = value + jnp.dot(block, W[w], preferred_element_type=F32)
            ACC[rows, :] = value
            return 0

        lax.fori_loop(0, 2, step, 0)

    def within(j):
        return (j >= 0) & (j < C)

    def pick(j, r):
        part = pl.ds(4 * r, 4)
        block = jnp.dot(
            S[part].reshape(4 * ROWS, NZ * TOK), G[j].reshape(NZ * TOK, FC), preferred_element_type=F32
        ).astype(BF16)
        XS[j, part] = block.reshape(4, ROWS, FC)
        for i in range(4):

            @pl.when(4 * r + i != q)
            def _():
                x_copy(j, 4 * r + i).start()

    def forward(t, s):
        j = t - s
        if s < 3:
            for d in range(2):

                @pl.when(j == 0)
                def _():
                    i_copy(s - 1, d).wait_recv()
                    i_copy(s, d).start()

                z_copy(j, s - 1, d).wait_recv()
                z_copy(j, s, d).start()
            return

        @pl.when(j == 0)
        def _():
            i_copy(2, 0).wait_recv()
            i_copy(2, 1).wait_recv()
            i_copy(3, 0).start()

        for d in range(2):
            z_copy(j, 2, d).wait_recv()

            @pl.when(lax.rem(j, 2) == d)
            def _():
                z_copy(j, 3, d).start()

    def gather(j):
        for d in range(2):

            @pl.when(lax.rem(j, 2) == d)
            def _():
                z_copy(j, 3, d).wait_recv()

        def step(r, _):
            pick(j, r)
            return 0

        lax.fori_loop(0, 2, step, 0)
        XF[j, q] = XS[j, q]

    def tick(t, _):
        for s in (3, 2, 1):

            @pl.when((t < 4) & within(t - s))
            def _():
                forward(t, s)

        @pl.when(t == 4)
        def _():
            i_copy(3, 0).wait_recv()
            build_gather()
            gather(0)

        for s in (1, 2, 3):

            @pl.when((t >= 4) & within(t - s))
            def _():
                forward(t, s)

        @pl.when(t == 1)
        def _():
            for d in range(2):
                z_copy(AHEAD, 0, d).start()

        @pl.when((t > 0) & (t + AHEAD < C))
        def _():
            for d in range(2):
                z_copy(t + AHEAD, 0, d).start()

        @pl.when((t > 4) & within(t - 4))
        def _():
            gather(t - 4)

        @pl.when(within(t - 6))
        def _():
            j = t - 6
            wait_bytes(XF.at[j, pl.ds(0, NQ - 1)], xrs.at[j])

            @pl.when(j < CE)
            def _():
                for d in range(2):
                    y_copy(j, d).start()

            @pl.when(j == 0)
            def _():
                loads[7].wait()
                loads[8].wait()

        @pl.when((t >= 6) & (t < 8))
        def _():
            expert_dots((XF, t - 6, chunk(t - 6)))

        @pl.when((t >= 8) & (t < 8 + CE))
        def _():
            j = t - 8
            wait_bytes(XO.at[j], yrs.at[j])
            expert_dots((XF, t - 6, chunk(t - 6)), (XO, j, (1 - half) * CE + j))

        @pl.when(t == 0)
        def _():
            own_windows()

        @pl.when(t == 2)
        def _():
            prior_windows()

        @pl.when((t == 1) | (t == 2))
        def _():
            for i in range(4):
                attend((2 - t) * 4 + i)

        @pl.when(t == 3)
        def _():
            loads[9].wait()

        @pl.when((t == 3) | (t == 4))
        def _():
            for i in range(4):
                project((t - 3) * 4 + i)

        @pl.when(t == 4)
        def _():
            for d in range(2):
                m_copy(0, d).start()

        return 0

    lax.fori_loop(0, C + 6, tick, 0)

    def pair(b):
        chip, core = q // 2, lax.rem(q, 2)
        apart = (b > 0) & (b < 3)
        dx = jnp.where(b == 0, 2, jnp.where(b == 3, 0, 1))
        dc = jnp.where(apart, b - 1, 0)
        first = lax.rem(chip + dx, 4) * 2 + lax.rem(core + dc, 2)
        dx = jnp.where(apart, 3, dx)
        dc = jnp.where(apart, b - 1, 1)
        return first, lax.rem(chip + dx, 4) * 2 + lax.rem(core + dc, 2)

    def activate(hb, _):
        h, b = hb // 4, lax.rem(hb, 4)
        for qq in pair(b):
            rows = pl.ds(pl.multiple_of(qq * ROWS + h * HALF, 16), HALF)
            g = jnp.minimum(ACC[rows, 0:HID], CLAMP)
            u = jnp.clip(ACC[rows, HID : 2 * HID], -CLAMP, CLAMP) + 1.0
            ACT[y, h, qq] = (u * g * jax.nn.sigmoid(SLOPE * g)).astype(BF16)
            for i in (2, 1, 3):
                a_copy(h, qq, b, i).start()
        return 0

    lax.fori_loop(0, 8, activate, 0)
    build_combine()
    loads[10].wait()
    wait_bytes(DN.at[pl.ds(0, NY - 1)], drs.at[0])
    for d in range(2):
        wait_bytes(PM.at[d], mrs.at[d])
        to = wrap(y + 1, NY) if d == 0 else wrap(y - 1, NY)
        PT[to, d] = (PT[to, d].astype(F32) + PM[d].astype(F32)).astype(BF16)

    def down(hb, _):
        h, b = hb // 4, lax.rem(hb, 4)
        wait_bytes(ACT.at[pl.ds(0, NY - 1), 0, pl.ds(0, 2)], ars.at[hb])
        qs = pair(b)
        block = jnp.zeros((2 * HALF, 1024), F32)
        for i in range(NY):
            acts = jnp.concatenate([ACT[i, h, qq] for qq in qs], axis=0)
            block = block + jnp.dot(acts, DN[i], preferred_element_type=F32)
        for i, qq in enumerate(qs):
            YS[h, qq] = block[i * HALF : (i + 1) * HALF].astype(BF16)

            @pl.when(qq != q)
            def _():
                w_copy(h, qq).start()

            @pl.when(qq == q)
            def _():
                RX[h, q] = YS[h, q]

        return 0

    lax.fori_loop(0, 5, down, 0)
    wait_bytes(RX.at[0, pl.ds(0, NQ - 1)], wrs.at[0])

    def partial_sum(n, place):
        cols = pl.ds(pl.multiple_of(n * FC, FC), FC)
        rows = RX[place // 4, :, :, cols].reshape(NQ * HALF, FC)
        return jnp.dot(CM[place], rows, preferred_element_type=F32)

    def send_sum(n, s, d):
        odd = lax.rem(n, 2)
        if d == 0:
            ahead = 4 - odd - s
            place = jnp.where(ahead == 4, 0, 2 * (4 - ahead) - 1)
        else:
            ahead = 3 + odd - s
            place = 2 * (4 - ahead)
        value = partial_sum(n, place)
        if s > 0:
            before = hop(s - 1, d)
            s_copy(n, before, d).wait_recv()
            value = value + RR[n, before].astype(F32)
        SR[n, hop(s, d)] = value.astype(BF16)
        s_copy(n, hop(s, d), d).start()

    def over_chunks(body):
        def step(n, _):
            body(n)
            return 0

        lax.fori_loop(0, NB, step, 0)

    def first(n):
        send_sum(n, 0, 0)
        send_sum(n, 0, 1)

    def most(s):
        def body(n):
            send_sum(n, s, 0)

            @pl.when(lax.rem(n, 2) == 1)
            def _():
                send_sum(n, s, 1)

        return body

    def rest(s):
        def body(n):
            @pl.when(lax.rem(n, 2) == 0)
            def _():
                send_sum(n, s, 1)

        return body

    def fourth(n):
        for d in range(2):

            @pl.when(lax.rem(n, 2) == d)
            def _():
                send_sum(n, 3, d)

    def finish(n):
        value = partial_sum(n, OWN)
        for d in range(2):
            last = jnp.where(lax.rem(n, 2) == d, 6, 4 + d)
            s_copy(n, last, d).wait_recv()
            value = value + RR[n, last].astype(F32)
        out_ref[:, pl.ds(pl.multiple_of(n * FC, FC), FC)] = value.astype(BF16)

    over_chunks(first)
    lax.fori_loop(5, 8, down, 0)
    for d in range(2):
        m_copy(1, d).start()
    over_chunks(most(1))
    wait_bytes(RX.at[1, pl.ds(0, NQ - 1)], wrs.at[1])
    over_chunks(rest(1))
    over_chunks(most(2))
    over_chunks(rest(2))
    over_chunks(fourth)

    wait_bytes(PN.at[0], mrs.at[2])
    wait_bytes(PN.at[1], mrs.at[3])

    def mix(u, _):
        c, cols = u // 4, pl.ds(pl.multiple_of(lax.rem(u, 4) * 512, 512), 512)
        value = PT[y, c, :, cols].astype(F32) + PN[0, c, :, cols].astype(F32) + PN[1, c, :, cols].astype(F32)
        mix_ref[:, pl.ds(pl.multiple_of(u * 512, 512), 512)] = value.astype(BF16)
        return 0

    lax.fori_loop(0, D // 512, mix, 0)
    over_chunks(finish)

    for view, sem in (
        (G.at[:, pl.ds(0, 7)], zss),
        (IR.at[pl.ds(0, 7)], iss),
        (XS.at[:, pl.ds(0, NQ - 1)], xss),
        (XO, yss),
        (DN.at[pl.ds(0, NY - 1)], dss),
        (ACT.at[pl.ds(0, NY - 1)], ass),
        (RX.at[:, pl.ds(0, NQ - 1)], wss),
        (SR, sss),
        (PM, mss),
        (KP, hss),
    ):
        wait_bytes(view, sem.at[0])
    wait_bytes(PN, mss.at[1])


def shards(
    projected_queries,
    key_proj,
    projected_values,
    head_sink_logits,
    out_weight,
    expert_input,
    norm_gain,
    routing,
    route_weight,
    gate_weight,
    up_weight,
    down_weight,
):
    vmem = pl.BlockSpec(memory_space=pltpu.VMEM)
    hbm = pl.BlockSpec(memory_space=pl.ANY)
    smem = pl.BlockSpec(memory_space=pltpu.SMEM)
    dma = pltpu.SemaphoreType.DMA
    mixed, combined = pl.pallas_call(
        kernel,
        out_shape=(
            pltpu.VMEM((64, D), BF16),
            pltpu.VMEM((TOK, 1024), BF16),
        ),
        in_specs=[hbm, hbm, hbm, smem, hbm, hbm, hbm, hbm, hbm, hbm, hbm, hbm],
        out_specs=(vmem, vmem),
        scratch_shapes=[
            pltpu.VMEM((256, 512), BF16),
            pltpu.VMEM((256, 128), BF16),
            pltpu.VMEM((256, 128), BF16),
            pltpu.VMEM((TOK, D), BF16),
            pltpu.VMEM((1, D), F32),
            pltpu.VMEM((4, TOK), jnp.int32),
            pltpu.VMEM((4, TOK), F32),
            pltpu.VMEM((C, NZ, TOK, FC), BF16),
            pltpu.VMEM((C, NQ, ROWS, FC), BF16),
            pltpu.VMEM((C, NQ, ROWS, FC), BF16),
            pltpu.VMEM((CE, NQ, ROWS, FC), BF16),
            pltpu.VMEM((D // FC, FC, 2 * HID), BF16),
            pltpu.VMEM((512, D), BF16),
            pltpu.VMEM((NY, HID, 1024), BF16),
            pltpu.VMEM((NQ, ROWS, NZ * TOK), BF16),
            pltpu.VMEM((NZ, TOK, NQ * HALF), BF16),
            pltpu.VMEM((NZ, 8, TOK), F32),
            pltpu.VMEM((NZ, 16, TOK), F32),
            pltpu.VMEM((NQ * ROWS, 2 * HID), F32),
            pltpu.VMEM((NY, 2, NQ, HALF, HID), BF16),
            pltpu.VMEM((2, NQ, HALF, 1024), BF16),
            pltpu.VMEM((2, NQ, HALF, 1024), BF16),
            pltpu.VMEM((NB, 7, TOK, FC), BF16),
            pltpu.VMEM((NB, 7, TOK, FC), BF16),
            pltpu.VMEM((2, 128, 128), BF16),
            pltpu.VMEM((2, 2, 384, 128), BF16),
            pltpu.VMEM((2, 2, 384, 128), BF16),
            pltpu.VMEM((256, 512), BF16),
            pltpu.VMEM((NY, 2, 64, D // 2), BF16),
            pltpu.VMEM((2, 64, D // 2), BF16),
            pltpu.VMEM((2, 2, 64, D // 2), BF16),
            dma((11,)),
            dma((1,)), dma((C, 7)),
            dma((1,)), dma((7,)),
            dma((1,)), dma((C,)),
            dma((1,)), dma((CE,)),
            dma((1,)), dma((1,)),
            dma((1,)), dma((8,)),
            dma((1,)), dma((2,)),
            dma((1,)), dma((NB, 7)),
            dma((2,)), dma((4,)),
            dma((1,)), dma((1,)),
        ],
        compiler_params=pltpu.CompilerParams(
            collective_id=0, has_side_effects=True, vmem_limit_bytes=62 * 1024 * 1024
        ),
    )(
        projected_queries,
        key_proj,
        projected_values,
        head_sink_logits,
        out_weight,
        expert_input,
        norm_gain.reshape(1, D),
        routing.T,
        route_weight.T,
        gate_weight.reshape(D // FC, FC, HID),
        up_weight.reshape(D // FC, FC, HID),
        down_weight.reshape(HID, D),
    )
    return mixed, combined


def solution(mesh):
    placed = (
        P("ep", "tp"),
        P("ep", "tp"),
        P("ep", "tp"),
        P("tp"),
        P("tp", None),
        P("ep", None),
        P(),
        P("ep", None),
        P("ep", None),
        P("ep", None, "tp"),
        P("ep", None, "tp"),
        P("ep", "tp", None),
    )
    return jax.shard_map(
        shards,
        mesh=mesh,
        in_specs=placed,
        out_specs=(P(("ep", "tp"), None), P("ep", "tp")),
        check_vma=False,
    )
```

```python
import jax
import jax.numpy as jnp
from jax import lax
from jax.experimental import pallas as pl
from jax.experimental.pallas import tpu as pltpu
from jax.sharding import PartitionSpec as P

EPS = 1e-06
CLAMP = 7.0
SLOPE = 1.702

NZ = 8
NQ = 8
NY = 4
D = 4096
TOK = 128
CAP = 12
ROWS = NZ * CAP
FC = 256
CE = 7
C = 9
AHEAD = 2
HID = 256
NB = 4
HALF = ROWS // 2
PLACE = (7, 5, 3, 1, 0, 2, 4, 6)
OWN = 7
MESH = pl.DeviceIdType.MESH
F32 = jnp.float32
BF16 = jnp.bfloat16


def kernel(
    q_hbm, k_hbm, v_hbm, sink_ref, wo_hbm, x_hbm, gain_hbm, rt_hbm, rw_hbm, wg_hbm, wu_hbm, wd_hbm,
    mix_ref, out_ref,
    q_ref, k_ref, v_ref, x_ref, gain_ref, rt_ref, rw_ref,
    G, XS, XF, XO, W, WO, DN, S, CM, IR, RANK, ACC, ACT, YS, RX, SR, RR,
    KP, KX, VX, ATT, PT, PM, PN,
    ls, zss, zrs, iss, irs, xss, xrs, yss, yrs, dss, drs, ass, ars, wss, wrs, sss, srs, mss, mrs, hss, hrs,
):
    ep = lax.axis_index("ep")
    y = lax.axis_index("tp")
    z = ep // NQ
    q = lax.rem(ep, NQ)
    half = lax.rem(y, 2)

    def wrap(a, n):
        return lax.rem(a + n, n)

    def at_z(zz):
        return (zz * NQ + q, y)

    def at_q(qq):
        return (z * NQ + qq, y)

    def at_y(yy):
        return (ep, yy)

    def remote(src, dst, ss, rs, dev):
        return pltpu.make_async_remote_copy(src, dst, ss, rs, device_id=dev, device_id_type=MESH)

    barrier = pltpu.get_barrier_semaphore()
    next_ep, prev_ep = wrap(ep + 1, NZ * NQ), wrap(ep - 1, NZ * NQ)
    for i in (1, NZ - 1):
        pl.semaphore_signal(barrier, inc=1, device_id=at_z(wrap(z + i, NZ)), device_id_type=MESH)
    for i in range(1, NQ):
        pl.semaphore_signal(barrier, inc=1, device_id=at_q(wrap(q + i, NQ)), device_id_type=MESH)
    for i in range(1, NY):
        pl.semaphore_signal(barrier, inc=1, device_id=at_y(wrap(y + i, NY)), device_id_type=MESH)
    for e in (next_ep, prev_ep):
        pl.semaphore_signal(barrier, inc=1, device_id=(e, y), device_id_type=MESH)

    own_down = wd_hbm.at[:, pl.ds(pl.multiple_of(y * 1024, 1024), 1024)]
    pairs = (
        (x_hbm, x_ref), (gain_hbm, gain_ref), (rt_hbm, rt_ref), (rw_hbm, rw_ref),
        (k_hbm, k_ref), (v_hbm, v_ref), (q_hbm, q_ref),
        (wg_hbm, W.at[:, :, pl.ds(0, HID)]), (wu_hbm, W.at[:, :, pl.ds(HID, HID)]), (wo_hbm, WO), (own_down, DN.at[y]),
    )
    loads = [pltpu.make_async_copy(src, dst, ls.at[i]) for i, (src, dst) in enumerate(pairs)]
    for load in loads:
        load.start()

    def chunk(j):
        return jnp.where(j < CE, half * CE + j, CE + j)

    loads[0].wait()

    def mean_step(j, total):
        w = x_ref[:, pl.ds(pl.multiple_of(j * 512, 512), 512)].astype(F32)
        w = w * w
        return total + ((w[:, 0:128] + w[:, 128:256]) + (w[:, 256:384] + w[:, 384:512]))

    total = lax.fori_loop(0, D // 512, mean_step, jnp.zeros((TOK, 128), F32))
    scale = lax.rsqrt(jnp.sum(total, axis=1, keepdims=True) * (1.0 / D) + EPS)
    for i in (1, 2, 3):
        loads[i].wait()

    def norm_step(j, _):
        cols = pl.ds(pl.multiple_of(chunk(j) * FC, FC), FC)
        G[j, OWN] = (x_ref[:, cols].astype(F32) * scale * gain_ref[:, cols]).astype(BF16)
        return 0

    lax.fori_loop(0, C, norm_step, 0)
    IR[OWN] = jnp.concatenate([rt_ref[...].astype(F32), rw_ref[...]], axis=0)

    def hop(s, d):
        return 6 if s == 3 else 2 * s + d

    def ring(s, d):
        if d == 0:
            return PLACE[-s % NZ], PLACE[-(s + 1) % NZ], at_z(wrap(z + 1, NZ))
        return PLACE[s], PLACE[s + 1], at_z(wrap(z - 1, NZ))

    def z_copy(j, s, d):
        here, there, to = ring(s, d)
        return remote(G.at[j, here], G.at[j, there], zss.at[0], zrs.at[j, hop(s, d)], to)

    def i_copy(s, d):
        here, there, to = ring(s, d)
        return remote(IR.at[here], IR.at[there], iss.at[0], irs.at[hop(s, d)], to)

    def x_copy(j, to):
        return remote(XS.at[j, to], XF.at[j, q], xss.at[0], xrs.at[j], at_q(to))

    def y_copy(j, d):
        to = wrap(y + 1, NY) if d == 0 else wrap(y - 1, NY)
        part = pl.ds(4 * d, 4)
        return remote(XF.at[j, part], XO.at[j, part], yss.at[0], yrs.at[j], at_y(to))

    def d_copy(i):
        to = wrap(y + i, NY)
        src = wd_hbm.at[:, pl.ds(pl.multiple_of(to * 1024, 1024), 1024)]
        return remote(src, DN.at[y], dss.at[0], drs.at[0], at_y(to))

    def a_copy(h, qq, b, i):
        to = wrap(y + i, NY)
        return remote(ACT.at[y, h, qq], ACT.at[y, h, qq], ass.at[0], ars.at[8 * h + b], at_y(to))

    def w_copy(h, to):
        return remote(YS.at[h, to], RX.at[h, q], wss.at[0], wrs.at[h], at_q(to))

    def s_copy(n, h, d):
        peer = wrap(z + 1, NZ) if d == 0 else wrap(z - 1, NZ)
        return remote(SR.at[n, h], RR.at[n, h], sss.at[0], srs.at[n, h], at_z(peer))

    def m_copy(step, d):
        to = wrap(y + 1, NY) if d == 0 else wrap(y - 1, NY)
        if step == 0:
            return remote(PT.at[wrap(y + 2, NY), d], PM.at[d], mss.at[0], mrs.at[d], at_y(to))
        return remote(PT.at[to], PN.at[d], mss.at[1], mrs.at[2 + d], at_y(to))

    halo = [
        remote(k_hbm.at[pl.ds(128, 128)], KP.at[0], hss.at[0], hrs.at[0], (next_ep, y)),
        remote(v_hbm.at[pl.ds(128, 128)], KP.at[1], hss.at[0], hrs.at[0], (next_ep, y)),
    ]

    def wait_bytes(view, sem):
        pltpu.make_async_copy(view, view, sem).wait()

    pl.semaphore_wait(barrier, 2 + (NQ - 1) + (NY - 1) + 2)
    for d in range(2):
        z_copy(0, 0, d).start()
        i_copy(0, d).start()
    for j in range(1, AHEAD):
        for d in range(2):
            z_copy(j, 0, d).start()
    for copy in halo:
        copy.start()
    for i in (2, 1, 3):
        d_copy(i).start()
    ACC[...] = jnp.zeros_like(ACC)

    def widen(whole, wide, rows):
        lanes = lax.broadcasted_iota(jnp.int32, whole.shape, 1)
        whole = whole.astype(F32)
        turned = pltpu.roll(whole, 64, 1)
        zero = jnp.zeros_like(whole)
        wide[0, 0, rows, :] = jnp.where(lanes < 64, whole, zero).astype(BF16)
        wide[1, 1, rows, :] = jnp.where(lanes < 64, zero, whole).astype(BF16)
        wide[0, 1, rows, :] = jnp.where(lanes < 64, zero, turned).astype(BF16)
        wide[1, 0, rows, :] = jnp.where(lanes < 64, turned, zero).astype(BF16)

    def own_windows():
        for i in (4, 5, 6):
            loads[i].wait()
        widen(k_ref[...], KX, pl.ds(128, 256))
        widen(v_ref[...], VX, pl.ds(128, 256))

    def prior_windows():
        wait_bytes(KP, hrs.at[0])
        widen(KP[0], KX, pl.ds(0, 128))
        widen(KP[1], VX, pl.ds(0, 128))

    def div12(a):
        return (a * 5462) >> 16

    def build_gather():
        u = lax.broadcasted_iota(jnp.int32, (TOK, TOK), 0)
        t = lax.broadcasted_iota(jnp.int32, (TOK, TOK), 1)
        earlier = (u < t).astype(F32).astype(BF16)
        expert = (lax.broadcasted_iota(jnp.int32, (NQ, TOK), 0) + z * NQ).astype(F32)
        named, weight = [], []
        for zs in range(NZ):
            info = IR[zs]
            hits = [(info[k : k + 1, :] == expert).astype(F32) for k in range(4)]
            named.append(hits[0] + hits[1] + hits[2] + hits[3])
            weight.append(sum(hits[k] * info[4 + k : 5 + k, :] for k in range(4)))
        named = jnp.concatenate(named, axis=0)
        rank = jnp.dot(named.astype(BF16), earlier, preferred_element_type=F32)
        rank = jnp.where(named > 0.5, rank, -1.0)
        for zs in range(NZ):
            RANK[zs, 0:8, :] = rank[8 * zs : 8 * zs + 8, :]
            RANK[zs, 8:16, :] = weight[zs]
        row = lax.broadcasted_iota(jnp.int32, (ROWS, 128), 0)
        row_p = div12(row)
        row_k = (row - row_p * CAP).astype(F32)

        def step(zs, _):
            cols = pl.ds(pl.multiple_of(zs * TOK, TOK), TOK)
            ranks = RANK[zs, 0:8, :]
            for e in range(NQ):
                hit = (row_p == zs) & (ranks[e : e + 1, :] == row_k)
                S[e, :, cols] = hit.astype(F32).astype(BF16)
            return 0

        lax.fori_loop(0, NZ, step, 0)

    def build_combine():
        i16 = lax.broadcasted_iota(jnp.int32, (16, NQ * HALF), 0)
        col_q = div12(lax.broadcasted_iota(jnp.int32, (16, NQ * HALF), 1)) >> 2
        spread_rank = (i16 == col_q).astype(F32).astype(BF16)
        spread_weight = (i16 == col_q + 8).astype(F32).astype(BF16)
        col = lax.broadcasted_iota(jnp.int32, (TOK, NQ * HALF), 1)
        col12 = div12(col)
        col_p = col12 & 3
        col_k = (col - col12 * CAP).astype(F32)

        def step(p, _):
            turned = RANK[p].T.astype(BF16)
            ranks = jnp.dot(turned, spread_rank, preferred_element_type=F32)
            weights = jnp.dot(turned, spread_weight, preferred_element_type=F32)
            hit = (col_p == (p & 3)) & (ranks == col_k)
            CM[p] = jnp.where(hit, weights, 0.0).astype(BF16)
            return 0

        lax.fori_loop(0, NZ, step, 0)

    def attend(u):
        n, p = u // 4, lax.rem(u, 4)
        kv = p // 2
        rows = pl.ds(pl.multiple_of(n * 128, 128), 128)
        window = pl.ds(pl.multiple_of(n * 128, 128), 256)
        cols = pl.ds(pl.multiple_of(p * 128, 128), 128)
        queries = q_ref[rows, cols]
        i = lax.broadcasted_iota(jnp.int32, (128, 256), 0)
        s = lax.broadcasted_iota(jnp.int32, (128, 256), 1)
        first = jnp.where((ep == 0) & (n == 0), 128, 0)
        seen = (s > i) & (s <= i + 128) & (s >= first)
        both = jnp.zeros((128, 128), F32)
        for h in range(2):
            scores = lax.dot_general(
                queries, KX[kv, h, window, :], (((1,), (1,)), ((), ())), preferred_element_type=F32
            ) * 0.125
            scores = jnp.where(seen, scores, -jnp.inf)
            sink = sink_ref[2 * p + h]
            highest = jnp.maximum(jnp.max(scores, axis=1, keepdims=True), sink)
            e = jnp.exp(scores - highest)
            under = jnp.sum(e, axis=1, keepdims=True) + jnp.exp(sink - highest)
            w = (e / under).astype(BF16)
            both = both + jnp.dot(w, VX[kv, h, window, :], preferred_element_type=F32)
        ATT[rows, cols] = both.astype(BF16)

    def project(u):
        cols = pl.ds(pl.multiple_of(u * 512, 512), 512)
        part = jnp.dot(ATT[...], WO[:, cols], preferred_element_type=F32).astype(BF16)
        inner = pl.ds(pl.multiple_of(lax.rem(u, 4) * 512, 512), 512)
        PT[:, u // 4, :, inner] = part.reshape(NY, 64, 512)

    def expert_dots(*terms):
        def step(r, _):
            part = pl.ds(4 * r, 4)
            rows = pl.ds(pl.multiple_of(r * 4 * ROWS, 4 * ROWS), 4 * ROWS)
            value = ACC[rows, :]
            for src, j, w in terms:
                block = src[j, part].reshape(4 * ROWS, FC)
                value = value + jnp.dot(block, W[w], preferred_element_type=F32)
            ACC[rows, :] = value
            return 0

        lax.fori_loop(0, 2, step, 0)

    def within(j):
        return (j >= 0) & (j < C)

    def pick(j, r):
        part = pl.ds(4 * r, 4)
        block = jnp.dot(
            S[part].reshape(4 * ROWS, NZ * TOK), G[j].reshape(NZ * TOK, FC), preferred_element_type=F32
        ).astype(BF16)
        XS[j, part] = block.reshape(4, ROWS, FC)
        for i in range(4):

            @pl.when(4 * r + i != q)
            def _():
                x_copy(j, 4 * r + i).start()

    def forward(t, s):
        j = t - s
        if s < 3:
            for d in range(2):

                @pl.when(j == 0)
                def _():
                    i_copy(s - 1, d).wait_recv()
                    i_copy(s, d).start()

                z_copy(j, s - 1, d).wait_recv()
                z_copy(j, s, d).start()
            return

        @pl.when(j == 0)
        def _():
            i_copy(2, 0).wait_recv()
            i_copy(2, 1).wait_recv()
            i_copy(3, 0).start()

        for d in range(2):
            z_copy(j, 2, d).wait_recv()

            @pl.when(lax.rem(j, 2) == d)
            def _():
                z_copy(j, 3, d).start()

    def gather(j):
        for d in range(2):

            @pl.when(lax.rem(j, 2) == d)
            def _():
                z_copy(j, 3, d).wait_recv()

        def step(r, _):
            pick(j, r)
            return 0

        lax.fori_loop(0, 2, step, 0)
        XF[j, q] = XS[j, q]

    def tick(t, _):
        @pl.when(t == 4)
        def _():
            i_copy(3, 0).wait_recv()
            build_gather()
            gather(0)

        for s in (3, 2, 1):

            @pl.when((t <= 4) & within(t - s))
            def _():
                forward(t, s)

        for s in (1, 2, 3):

            @pl.when((t > 4) & within(t - s))
            def _():
                forward(t, s)

        @pl.when(t == 1)
        def _():
            for d in range(2):
                z_copy(AHEAD, 0, d).start()

        @pl.when((t > 0) & (t + AHEAD < C))
        def _():
            for d in range(2):
                z_copy(t + AHEAD, 0, d).start()

        @pl.when((t > 4) & within(t - 4))
        def _():
            gather(t - 4)

        @pl.when(t == C + 4)
        def _():
            build_combine()

        @pl.when(within(t - 6))
        def _():
            j = t - 6
            wait_bytes(XF.at[j, pl.ds(0, NQ - 1)], xrs.at[j])

            @pl.when(j < CE)
            def _():
                for d in range(2):
                    y_copy(j, d).start()

            @pl.when(j == 0)
            def _():
                loads[7].wait()
                loads[8].wait()

        @pl.when((t >= 6) & (t < 8))
        def _():
            expert_dots((XF, t - 6, chunk(t - 6)))

        @pl.when((t >= 8) & (t < 8 + CE))
        def _():
            j = t - 8
            wait_bytes(XO.at[j], yrs.at[j])
            expert_dots((XF, t - 6, chunk(t - 6)), (XO, j, (1 - half) * CE + j))

        @pl.when(t == 0)
        def _():
            own_windows()

        @pl.when(t == 2)
        def _():
            prior_windows()

        @pl.when((t == 1) | (t == 2))
        def _():
            for i in range(4):
                attend((2 - t) * 4 + i)

        @pl.when(t == 3)
        def _():
            loads[9].wait()

        @pl.when((t == 3) | (t == 4))
        def _():
            for i in range(4):
                project((t - 3) * 4 + i)

        @pl.when(t == 4)
        def _():
            for d in range(2):
                m_copy(0, d).start()

        return 0

    lax.fori_loop(0, C + 6, tick, 0)

    def nth(b):
        chip, core = q // 2, lax.rem(q, 2)
        turn, odd = b // 2, lax.rem(b, 2)
        apart = (turn > 0) & (turn < 3)
        dx = jnp.where(turn == 0, 2, jnp.where(turn == 3, 0, jnp.where(odd == 0, 1, 3)))
        dc = jnp.where(apart, turn - 1, odd)
        return lax.rem(chip + dx, 4) * 2 + lax.rem(core + dc, 2)

    def activate(hb, _):
        h, b = hb // 8, lax.rem(hb, 8)
        qq = nth(b)
        rows = pl.ds(pl.multiple_of(qq * ROWS + h * HALF, 16), HALF)
        g = jnp.minimum(ACC[rows, 0:HID], CLAMP)
        u = jnp.clip(ACC[rows, HID : 2 * HID], -CLAMP, CLAMP) + 1.0
        ACT[y, h, qq] = (u * g * jax.nn.sigmoid(SLOPE * g)).astype(BF16)
        for i in (2, 1, 3):
            a_copy(h, qq, b, i).start()
        return 0

    lax.fori_loop(0, 16, activate, 0)
    loads[10].wait()
    wait_bytes(DN.at[pl.ds(0, NY - 1)], drs.at[0])
    for d in range(2):
        wait_bytes(PM.at[d], mrs.at[d])
        to = wrap(y + 1, NY) if d == 0 else wrap(y - 1, NY)
        PT[to, d] = (PT[to, d].astype(F32) + PM[d].astype(F32)).astype(BF16)

    def down(hb, _):
        h, b = hb // 8, lax.rem(hb, 8)
        wait_bytes(ACT.at[pl.ds(0, NY - 1), 0, 0], ars.at[hb])
        qq = nth(b)
        block = jnp.zeros((HALF, 1024), F32)
        for i in range(NY):
            block = block + jnp.dot(ACT[i, h, qq], DN[i], preferred_element_type=F32)
        YS[h, qq] = block.astype(BF16)

        @pl.when(qq != q)
        def _():
            w_copy(h, qq).start()

        @pl.when(qq == q)
        def _():
            RX[h, q] = YS[h, q]

        return 0

    lax.fori_loop(0, 10, down, 0)
    wait_bytes(RX.at[0, pl.ds(0, NQ - 1)], wrs.at[0])

    def partial_sum(n, place):
        cols = pl.ds(pl.multiple_of(n * FC, FC), FC)
        rows = RX[place // 4, :, :, cols].reshape(NQ * HALF, FC)
        return jnp.dot(CM[place], rows, preferred_element_type=F32)

    def send_sum(n, s, d):
        odd = lax.rem(n, 2)
        if d == 0:
            ahead = 4 - odd - s
            place = jnp.where(ahead == 4, 0, 2 * (4 - ahead) - 1)
        else:
            ahead = 3 + odd - s
            place = 2 * (4 - ahead)
        value = partial_sum(n, place)
        if s > 0:
            before = hop(s - 1, d)
            s_copy(n, before, d).wait_recv()
            value = value + RR[n, before].astype(F32)
        SR[n, hop(s, d)] = value.astype(BF16)
        s_copy(n, hop(s, d), d).start()

    def over_chunks(body):
        def step(n, _):
            body(n)
            return 0

        lax.fori_loop(0, NB, step, 0)

    def first(n):
        send_sum(n, 0, 0)
        send_sum(n, 0, 1)

    def most(s):
        def body(n):
            send_sum(n, s, 0)

            @pl.when(lax.rem(n, 2) == 1)
            def _():
                send_sum(n, s, 1)

        return body

    def rest(s):
        def body(n):
            @pl.when(lax.rem(n, 2) == 0)
            def _():
                send_sum(n, s, 1)

        return body

    def fourth(n):
        for d in range(2):

            @pl.when(lax.rem(n, 2) == d)
            def _():
                send_sum(n, 3, d)

    def finish(n):
        value = partial_sum(n, OWN)
        for d in range(2):
            last = jnp.where(lax.rem(n, 2) == d, 6, 4 + d)
            s_copy(n, last, d).wait_recv()
            value = value + RR[n, last].astype(F32)
        out_ref[:, pl.ds(pl.multiple_of(n * FC, FC), FC)] = value.astype(BF16)

    over_chunks(first)
    lax.fori_loop(10, 16, down, 0)
    for d in range(2):
        m_copy(1, d).start()
    over_chunks(most(1))
    wait_bytes(RX.at[1, pl.ds(0, NQ - 1)], wrs.at[1])
    over_chunks(rest(1))
    over_chunks(most(2))
    over_chunks(rest(2))
    over_chunks(fourth)

    wait_bytes(PN.at[0], mrs.at[2])
    wait_bytes(PN.at[1], mrs.at[3])

    def mix(u, _):
        c, cols = u // 4, pl.ds(pl.multiple_of(lax.rem(u, 4) * 512, 512), 512)
        value = PT[y, c, :, cols].astype(F32) + PN[0, c, :, cols].astype(F32) + PN[1, c, :, cols].astype(F32)
        mix_ref[:, pl.ds(pl.multiple_of(u * 512, 512), 512)] = value.astype(BF16)
        return 0

    lax.fori_loop(0, D // 512, mix, 0)
    over_chunks(finish)

    for view, sem in (
        (G.at[:, pl.ds(0, 7)], zss),
        (IR.at[pl.ds(0, 7)], iss),
        (XS.at[:, pl.ds(0, NQ - 1)], xss),
        (XO, yss),
        (DN.at[pl.ds(0, NY - 1)], dss),
        (ACT.at[pl.ds(0, NY - 1)], ass),
        (RX.at[:, pl.ds(0, NQ - 1)], wss),
        (SR, sss),
        (PM, mss),
        (KP, hss),
    ):
        wait_bytes(view, sem.at[0])
    wait_bytes(PN, mss.at[1])


def shards(
    projected_queries,
    key_proj,
    projected_values,
    head_sink_logits,
    out_weight,
    expert_input,
    norm_gain,
    routing,
    route_weight,
    gate_weight,
    up_weight,
    down_weight,
):
    vmem = pl.BlockSpec(memory_space=pltpu.VMEM)
    hbm = pl.BlockSpec(memory_space=pl.ANY)
    smem = pl.BlockSpec(memory_space=pltpu.SMEM)
    dma = pltpu.SemaphoreType.DMA
    mixed, combined = pl.pallas_call(
        kernel,
        out_shape=(
            pltpu.VMEM((64, D), BF16),
            pltpu.VMEM((TOK, 1024), BF16),
        ),
        in_specs=[hbm, hbm, hbm, smem, hbm, hbm, hbm, hbm, hbm, hbm, hbm, hbm],
        out_specs=(vmem, vmem),
        scratch_shapes=[
            pltpu.VMEM((256, 512), BF16),
            pltpu.VMEM((256, 128), BF16),
            pltpu.VMEM((256, 128), BF16),
            pltpu.VMEM((TOK, D), BF16),
            pltpu.VMEM((1, D), F32),
            pltpu.VMEM((4, TOK), jnp.int32),
            pltpu.VMEM((4, TOK), F32),
            pltpu.VMEM((C, NZ, TOK, FC), BF16),
            pltpu.VMEM((C, NQ, ROWS, FC), BF16),
            pltpu.VMEM((C, NQ, ROWS, FC), BF16),
            pltpu.VMEM((CE, NQ, ROWS, FC), BF16),
            pltpu.VMEM((D // FC, FC, 2 * HID), BF16),
            pltpu.VMEM((512, D), BF16),
            pltpu.VMEM((NY, HID, 1024), BF16),
            pltpu.VMEM((NQ, ROWS, NZ * TOK), BF16),
            pltpu.VMEM((NZ, TOK, NQ * HALF), BF16),
            pltpu.VMEM((NZ, 8, TOK), F32),
            pltpu.VMEM((NZ, 16, TOK), F32),
            pltpu.VMEM((NQ * ROWS, 2 * HID), F32),
            pltpu.VMEM((NY, 2, NQ, HALF, HID), BF16),
            pltpu.VMEM((2, NQ, HALF, 1024), BF16),
            pltpu.VMEM((2, NQ, HALF, 1024), BF16),
            pltpu.VMEM((NB, 7, TOK, FC), BF16),
            pltpu.VMEM((NB, 7, TOK, FC), BF16),
            pltpu.VMEM((2, 128, 128), BF16),
            pltpu.VMEM((2, 2, 384, 128), BF16),
            pltpu.VMEM((2, 2, 384, 128), BF16),
            pltpu.VMEM((256, 512), BF16),
            pltpu.VMEM((NY, 2, 64, D // 2), BF16),
            pltpu.VMEM((2, 64, D // 2), BF16),
            pltpu.VMEM((2, 2, 64, D // 2), BF16),
            dma((11,)),
            dma((1,)), dma((C, 7)),
            dma((1,)), dma((7,)),
            dma((1,)), dma((C,)),
            dma((1,)), dma((CE,)),
            dma((1,)), dma((1,)),
            dma((1,)), dma((16,)),
            dma((1,)), dma((2,)),
            dma((1,)), dma((NB, 7)),
            dma((2,)), dma((4,)),
            dma((1,)), dma((1,)),
        ],
        compiler_params=pltpu.CompilerParams(
            collective_id=0, has_side_effects=True, vmem_limit_bytes=62 * 1024 * 1024
        ),
    )(
        projected_queries,
        key_proj,
        projected_values,
        head_sink_logits,
        out_weight,
        expert_input,
        norm_gain.reshape(1, D),
        routing.T,
        route_weight.T,
        gate_weight.reshape(D // FC, FC, HID),
        up_weight.reshape(D // FC, FC, HID),
        down_weight.reshape(HID, D),
    )
    return mixed, combined


def solution(mesh):
    placed = (
        P("ep", "tp"),
        P("ep", "tp"),
        P("ep", "tp"),
        P("tp"),
        P("tp", None),
        P("ep", None),
        P(),
        P("ep", None),
        P("ep", None),
        P("ep", None, "tp"),
        P("ep", None, "tp"),
        P("ep", "tp", None),
    )
    return jax.shard_map(
        shards,
        mesh=mesh,
        in_specs=placed,
        out_specs=(P(("ep", "tp"), None), P("ep", "tp")),
        check_vma=False,
    )
```
